32 devices in a mesh: sp: 8 (over z, x), tp: 4 (over y, core).
Axes of the slice: x: 2, y: 2, z: 4, core: 2. Of those that a mesh axis runs over, the one named last changes fastest.
Arguments:
- queries: bfloat16 [1024, 2048], P('sp', 'tp'), may hold values from -6 to 6
- key_rows: bfloat16 [1024, 2048], P('sp', 'tp'), may hold values from -6 to 6
- value_rows: bfloat16 [1024, 2048], P('sp', 'tp'), may hold values from -6 to 6
- gate_input: bfloat16 [1024, 2048], P('sp', 'tp'), may hold values from -6 to 6
- log_decay: float32 [1024, 16], P('sp', 'tp'), may hold values from -0.6 to 0, as said below
- head_gain: float32 [2048], P('tp'), may hold values from 0.1 to 1.9
- out_weight: bfloat16 [2048, 2048], P('tp'), may hold values from -0.125 to 0.125
- residual: bfloat16 [1024, 2048], P('sp'), may hold values from -6 to 6
- mlp_gain: float32 [2048], replicated, may hold values from 0.1 to 1.9
- gate_weight: bfloat16 [2048, 5632], P('sp', 'tp'), may hold values from -0.125 to 0.125
- up_weight: bfloat16 [2048, 5632], P('sp', 'tp'), may hold values from -0.125 to 0.125
- down_weight: bfloat16 [5632, 2048], P('tp', 'sp'), may hold values from -0.078125 to 0.078125
Outputs:
- layer_out: bfloat16 [1024, 2048], P(('sp', 'tp'))
The draws below stay inside these ranges and needn't reach their ends.
Inputs may be any that keep to these rules, and one draw needn't show every extreme that they name: log_decay holds the logarithm of a decay factor of each head at each position.
All inputs are finite; a program needn't handle non-finite values.
Results may differ from the reference program's by a relative error of at most 0.017.
Values may be sent and summed in bfloat16 or wider, within the bound.
A program may use at most 128 MiB of HBM per device.

```python
import math
import jax
import jax.numpy as jnp
from jax import lax

D = 2048
RETENTION_HEADS = 16
HD = 128
FF = 5632
BLOCK = 128
TOK_DEV = 128
SEQUENCE_TOKENS = 1024
N_TP = 4


def draw_log_decay(key, part):
    key_collection = jax.random.split(jax.random.fold_in(key, 11), 5)
    slow_kind = jax.random.randint(key_collection[0], (RETENTION_HEADS,), 0, 10) < 5
    fast_length = jnp.exp(jax.random.uniform(key_collection[1], (RETENTION_HEADS,), jnp.float32, math.log(30.0), math.log(100.0)))
    fast_rate = -1.0 / fast_length
    device_blocks = SEQUENCE_TOKENS // TOK_DEV
    factor = jnp.exp(jax.random.uniform(key_collection[2], (device_blocks, RETENTION_HEADS), jnp.float32, math.log(0.4), math.log(1.6)))
    slow_rate = jnp.repeat(factor, TOK_DEV, axis=0) * (-0.4 / SEQUENCE_TOKENS)
    spike_positions = jax.random.randint(key_collection[3], (3, RETENTION_HEADS), 0, SEQUENCE_TOKENS)
    spike_length = jnp.log(jax.random.uniform(key_collection[4], (3, RETENTION_HEADS), jnp.float32, 0.6, 0.8))
    token_spots = jnp.arange(SEQUENCE_TOKENS, dtype=jnp.int32)[:, None, None]
    spike_rows = jnp.sum(jnp.where(token_spots == spike_positions[None], spike_length[None], 0.0), axis=1)
    constant_level = jnp.where(slow_kind[None, :], slow_rate, fast_rate[None, :])
    return (constant_level + spike_rows).astype(jnp.float32)


def levels(rng, shape, cuts, smallest, high):
    level = 1.0
    for dim, parts in cuts:
        heights = jax.random.uniform(jax.random.fold_in(jax.random.fold_in(rng, 6), dim), (parts,), jnp.float32, smallest / len(cuts), high / len(cuts))
        level = level * jnp.repeat(jnp.exp(heights), shape[dim] // parts).reshape((-1,) + (1,) * (len(shape) - 1 - dim))
    return level


def gaussian(own_key, shape, scale, reach, pieces=(), kind=jnp.bfloat16):
    drawn = scale * jax.random.normal(own_key, shape, jnp.float32)
    if pieces:
        drawn = drawn * levels(own_key, shape, pieces, -0.22, 0.18)
    return jnp.clip(drawn, -reach, reach).astype(kind)


def setup_inputs(seed: int = 0) -> dict:
    streams_of = jax.random.split(jax.random.key(seed), 13)
    return {
        "queries": gaussian(streams_of[0], (SEQUENCE_TOKENS, RETENTION_HEADS * HD), 1.0, 6.0, ((0, 8), (1, 4))),
        "key_rows": gaussian(streams_of[1], (SEQUENCE_TOKENS, RETENTION_HEADS * HD), 1.0, 6.0, ((0, 8), (1, 4))),
        "value_rows": gaussian(streams_of[2], (SEQUENCE_TOKENS, RETENTION_HEADS * HD), 1.0, 6.0, ((0, 8), (1, 4))),
        "gate_input": gaussian(streams_of[3], (SEQUENCE_TOKENS, RETENTION_HEADS * HD), 1.0, 6.0, ((0, 8), (1, 4))),
        "log_decay": draw_log_decay(jax.random.fold_in(streams_of[12], 71), 0),
        "head_gain": jnp.clip(1.0 + 0.18 * jax.random.normal(streams_of[5], (RETENTION_HEADS * HD,), jnp.float32), 0.1, 1.9),
        "out_weight": gaussian(streams_of[6], (RETENTION_HEADS * HD, D), (RETENTION_HEADS * HD) ** -0.5, 0.125, ((0, 4),)),
        "residual": gaussian(streams_of[7], (SEQUENCE_TOKENS, D), 1.0, 6.0, ((0, 8),)),
        "mlp_gain": jnp.clip(1.0 + 0.18 * jax.random.normal(streams_of[8], (D,), jnp.float32), 0.1, 1.9),
        "gate_weight": gaussian(streams_of[9], (D, FF), D ** -0.5, 0.125, ((0, 8), (1, 4))),
        "up_weight": gaussian(streams_of[10], (D, FF), D ** -0.5, 0.125, ((0, 8), (1, 4))),
        "down_weight": gaussian(streams_of[11], (FF, D), FF ** -0.5, 0.078125, ((0, 4), (1, 8))),
    }


EPS = 1e-06

def rotate(values_in, positions):
    half = values_in.shape[-1] // 2
    freq = 10000.0 ** (-jnp.linspace(0.0, 1.0, half, dtype=jnp.float32))
    angles = positions * freq
    angles = jnp.concatenate([angles, angles], axis=-1)
    first = values_in[..., :half]
    second = values_in[..., half:]
    turned = jnp.concatenate([-second, first], axis=-1)
    return values_in * jnp.cos(angles) + turned * jnp.sin(angles)

def row_norm(stream, gain):
    return stream * lax.rsqrt(lax.optimization_barrier(jnp.mean(stream * stream, axis=-1, keepdims=True)) + EPS) * gain

def retain_head(inputs):
    query_head, key_head, value_head, decay_head, gain_head = inputs
    length = query_head.shape[0]
    positions = jnp.arange(length, dtype=jnp.float32)[:, None]
    q_rot = rotate(query_head.astype(jnp.float32), positions).astype(jnp.bfloat16)
    k_rot = (rotate(key_head.astype(jnp.float32), positions) * HD ** (-0.5)).astype(jnp.bfloat16)
    blocks = length // BLOCK
    q_blocks = q_rot.reshape(blocks, BLOCK, HD).astype(jnp.float32)
    k_blocks = k_rot.reshape(blocks, BLOCK, HD).astype(jnp.float32)
    v_blocks = value_head.reshape(blocks, BLOCK, HD).astype(jnp.float32)
    cumul = jnp.cumsum(decay_head.reshape(blocks, BLOCK), axis=1)
    lower = jnp.tril(jnp.ones((BLOCK, BLOCK), dtype=bool))
    spread = cumul[:, :, None] - cumul[:, None, :]
    weight = jnp.where(lower, jnp.exp(jnp.where(lower, spread, 0.0)), 0.0)
    scores = jnp.einsum('ntd,nsd->nts', q_blocks, k_blocks)
    probs = (scores * weight).astype(jnp.bfloat16).astype(jnp.float32)
    inner = jnp.einsum('nts,nse->nte', probs, v_blocks)
    k_weighted = (k_blocks * jnp.exp(cumul[:, -1:] - cumul)[:, :, None]).astype(jnp.bfloat16).astype(jnp.float32)
    contrib = jnp.einsum('nsd,nse->nde', k_weighted, v_blocks)
    totals = jnp.exp(cumul[:, -1])

    def advance(state, items):
        factor, update = items
        return (state * factor + update, state)
    _, before = lax.scan(advance, jnp.zeros((HD, HD), jnp.float32), (totals, contrib))
    cross = jnp.einsum('ntd,nde->nte', q_blocks, before, precision=lax.Precision.HIGHEST)
    cross = cross * jnp.exp(cumul)[:, :, None]
    result = (inner + cross).reshape(length, HD)
    return row_norm(result, gain_head)

def reference(queries, key_rows, value_rows, gate_input, log_decay, head_gain, out_weight, residual, mlp_gain, gate_weight, up_weight, down_weight):

    def by_head(array):
        return array.reshape(SEQUENCE_TOKENS, RETENTION_HEADS, HD).transpose(1, 0, 2)
    heads_out = lax.map(retain_head, (by_head(queries), by_head(key_rows), by_head(value_rows), log_decay.T, head_gain.reshape(RETENTION_HEADS, HD)))
    joined = heads_out.transpose(1, 0, 2).reshape(SEQUENCE_TOKENS, RETENTION_HEADS * HD)
    gate_act = jax.nn.silu(gate_input.astype(jnp.float32))
    retained = (joined * gate_act).astype(jnp.bfloat16)
    width = RETENTION_HEADS * HD // N_TP
    hidden_width = FF // N_TP

    def layer_block(items):
        ret_rows, res_rows = items
        mixed = jnp.zeros((TOK_DEV, D), jnp.float32)
        for group_idx in range(N_TP):
            part = jnp.dot(ret_rows[:, group_idx * width:(group_idx + 1) * width], out_weight[group_idx * width:(group_idx + 1) * width], preferred_element_type=jnp.float32)
            part = lax.optimization_barrier(part.astype(jnp.bfloat16))
            mixed = mixed + part.astype(jnp.float32)
        middle = (res_rows.astype(jnp.float32) + mixed).astype(jnp.bfloat16)
        normed = row_norm(middle.astype(jnp.float32), mlp_gain).astype(jnp.bfloat16)
        gate = jnp.dot(normed, gate_weight, preferred_element_type=jnp.float32)
        upvals = jnp.dot(normed, up_weight, preferred_element_type=jnp.float32)
        hidden = (jax.nn.silu(gate) * upvals).astype(jnp.bfloat16)
        ffn = jnp.zeros((TOK_DEV, D), jnp.float32)
        for group_idx in range(N_TP):
            part = jnp.dot(hidden[:, group_idx * hidden_width:(group_idx + 1) * hidden_width], down_weight[group_idx * hidden_width:(group_idx + 1) * hidden_width], preferred_element_type=jnp.float32)
            part = lax.optimization_barrier(part.astype(jnp.bfloat16))
            ffn = ffn + part.astype(jnp.float32)
        return (middle.astype(jnp.float32) + ffn).astype(jnp.bfloat16)
    outcome = lax.map(layer_block, (retained.reshape(-1, TOK_DEV, RETENTION_HEADS * HD), residual.reshape(-1, TOK_DEV, D)))
    return outcome.reshape(SEQUENCE_TOKENS, D)
```

```python
import functools
import math
import types

import jax
import jax.numpy as jnp
from jax import lax
from jax.experimental import pallas as pl
from jax.experimental.pallas import tpu as pltpu
from jax.sharding import PartitionSpec as P

BLOCK = 128


EPS = 1e-06


def prefix_2(x, axis, join, neutral):
    place = lax.axis_index(axis)
    gathered = jax.tree.map(
        lambda a, kind: lax.all_gather(a.astype(kind), axis), x, (jnp.bfloat16, jnp.bfloat16)
    )
    state = jax.tree.map(lambda a, e: jnp.zeros_like(a) + jnp.asarray(e, a.dtype), x, neutral)

    def one(step, state):
        return join(
            state,
            jax.tree.map(
                lambda a, own: lax.dynamic_index_in_dim(a, step, 0, False).astype(own.dtype),
                gathered,
                x,
            ),
        )

    return lax.fori_loop(0, place, one, state)


def rotate(values_in, positions):
    half = values_in.shape[-1] // 2
    freq = 10000.0 ** (-jnp.linspace(0.0, 1.0, half, dtype=jnp.float32))
    angles = positions * freq
    angles = jnp.concatenate([angles, angles], axis=-1)
    first = values_in[..., :half]
    second = values_in[..., half:]
    turned = jnp.concatenate([-second, first], axis=-1)
    return values_in * jnp.cos(angles) + turned * jnp.sin(angles)


def row_norm(stream, gain):
    return stream * lax.rsqrt(jnp.mean(stream * stream, axis=-1, keepdims=True) + EPS) * gain


def join_states(earlier, later):
    return (earlier[0] * later[0], later[0][:, None, None] * earlier[1] + later[1])


def body(
    queries,
    key_rows,
    value_rows,
    gate_input,
    log_decay,
    head_gain,
    out_weight,
    residual,
    mlp_gain,
    gate_weight,
    up_weight,
    down_weight,
):
    tok_rows = queries.shape[0]
    heads_here = log_decay.shape[1]
    head_size = head_gain.shape[0] // heads_here
    quarter = tok_rows // lax.axis_size("tp")
    offset = lax.axis_index("sp") * tok_rows
    positions = (offset + lax.iota(jnp.int32, tok_rows)).astype(jnp.float32)[:, None, None]
    q_rot = rotate(
        queries.reshape(tok_rows, heads_here, head_size).astype(jnp.float32), positions
    ).astype(jnp.bfloat16)
    k_rot = (
        rotate(key_rows.reshape(tok_rows, heads_here, head_size).astype(jnp.float32), positions)
        * head_size ** (-0.5)
    ).astype(jnp.bfloat16)
    blocks = tok_rows // BLOCK
    q_blocks = q_rot.reshape(blocks, BLOCK, heads_here, head_size)
    k_blocks = k_rot.reshape(blocks, BLOCK, heads_here, head_size)
    v_blocks = value_rows.reshape(blocks, BLOCK, heads_here, head_size)
    cumul = jnp.cumsum(log_decay.reshape(blocks, BLOCK, heads_here), axis=1)
    by_head = cumul.transpose(0, 2, 1)
    lower = jnp.tril(jnp.ones((BLOCK, BLOCK), dtype=bool))
    spread = by_head[:, :, :, None] - by_head[:, :, None, :]
    weight = jnp.where(lower, jnp.exp(jnp.where(lower, spread, 0.0)), 0.0)
    scores = jnp.einsum("nthd,nshd->nhts", q_blocks, k_blocks, preferred_element_type=jnp.float32)
    probs = (scores * weight).astype(jnp.bfloat16)
    inner = jnp.einsum("nhts,nshe->nthe", probs, v_blocks, preferred_element_type=jnp.float32)
    k_weighted = (
        k_blocks.astype(jnp.float32) * jnp.exp(cumul[:, -1:, :] - cumul)[..., None]
    ).astype(jnp.bfloat16)
    contrib = jnp.einsum(
        "nshd,nshe->nhde", k_weighted, v_blocks, preferred_element_type=jnp.float32
    )
    totals = jnp.exp(cumul[:, -1, :])

    def advance(carry, items):
        state, prefix = carry
        factor, update = items
        return ((state * factor[:, None, None] + update, prefix * factor), (state, prefix))

    start_state = jnp.zeros((heads_here, head_size, head_size), jnp.float32)
    start_prefix = jnp.ones((heads_here,), jnp.float32)
    (dev_state, dev_total), (local_before, prefixes) = lax.scan(
        advance, (start_state, start_prefix), (totals, contrib)
    )
    _, incoming = prefix_2((dev_total, dev_state), "sp", join_states, (start_prefix, start_state))
    before = local_before + prefixes[:, :, None, None] * incoming[None]
    cross = jnp.einsum(
        "nthd,nhde->nthe", q_blocks.astype(jnp.float32), before, precision=lax.Precision.HIGHEST
    )
    cross = cross * jnp.exp(cumul)[..., None]
    result = (inner + cross).reshape(tok_rows, heads_here, head_size)
    result = row_norm(result, head_gain.reshape(heads_here, head_size)).reshape(
        tok_rows, heads_here * head_size
    )
    retained = (result * jax.nn.silu(gate_input.astype(jnp.float32))).astype(jnp.bfloat16)
    picked = retained
    mixed = lax.psum_scatter(
        jnp.dot(picked, out_weight, preferred_element_type=jnp.float32).astype(jnp.bfloat16),
        "tp",
        scatter_dimension=0,
        tiled=True,
    ).astype(jnp.float32)
    own_rows = lax.dynamic_slice_in_dim(residual, lax.axis_index("tp") * quarter, quarter, 0)
    rows_mid = (own_rows.astype(jnp.float32) + mixed).astype(jnp.bfloat16)
    own_normed = row_norm(rows_mid.astype(jnp.float32), mlp_gain).astype(jnp.bfloat16)
    normed = lax.all_gather(own_normed, "tp", axis=0, tiled=True)
    gate = jnp.dot(
        normed,
        lax.all_gather(gate_weight, "sp", axis=0, tiled=True),
        preferred_element_type=jnp.float32,
    )
    upvals = jnp.dot(
        normed,
        lax.all_gather(up_weight, "sp", axis=0, tiled=True),
        preferred_element_type=jnp.float32,
    )
    full_down = lax.all_gather(down_weight, "sp", axis=1, tiled=True)
    hidden = (jax.nn.silu(gate) * upvals).astype(jnp.bfloat16)
    picked = hidden
    ffn = lax.psum_scatter(
        jnp.dot(picked, full_down, preferred_element_type=jnp.float32).astype(jnp.bfloat16),
        "tp",
        scatter_dimension=0,
        tiled=True,
    ).astype(jnp.float32)
    return (rows_mid.astype(jnp.float32) + ffn).astype(jnp.bfloat16)


MESH = pl.DeviceIdType.MESH
XS = 2
CS = 2
F32 = jnp.float32
BF16 = jnp.bfloat16


def dot_nt(a, b):
    return lax.dot_general(a, b, (((1,), (1,)), ((), ())), preferred_element_type=F32)


def dot_nn(a, b):
    return lax.dot_general(a, b, (((1,), (0,)), ((), ())), preferred_element_type=F32)


def kernel(names, nz, nt, *refs):
    r = types.SimpleNamespace(**dict(zip(names, refs)))
    sp = lax.axis_index("sp")
    tp = lax.axis_index("tp")
    z, x = sp // XS, lax.rem(sp, XS)
    y, c = tp // CS, lax.rem(tp, CS)
    rows = r.q.shape[0]
    heads = r.ld.shape[0]
    hh = heads // XS
    hd = r.q.shape[1] // heads
    quarter = rows // nt
    share, width = r.wg.shape[2], r.wg.shape[3]
    group = XS * width
    ns = nz * XS
    zat = [z, z + 1 - 2 * lax.rem(z, 2), lax.rem(z + 2, nz), nz - 1 - z]

    def dev(zz, xx, yy, cc):
        return (zz * XS + xx, yy * CS + cc)

    x_peer = dev(z, 1 - x, y, c)
    c_peer = dev(z, x, y, 1 - c)

    barrier = pltpu.get_barrier_semaphore()
    peers = [dev(zat[e], x, y, k) for e in range(1, nz) for k in range(CS)]
    peers += [c_peer, dev(zat[2], 1 - x, y, c), dev(zat[1], x, 1 - y, c)]
    peers += [dev(z, 1 - x, y, k) for k in range(CS)]
    peers += [dev(z, x, 1 - y, k) for k in range(CS)]
    for peer in peers:
        pl.semaphore_signal(barrier, inc=1, device_id=peer, device_id_type=MESH)

    loads = {}

    def load(name, src, dst):
        loads[name] = pltpu.make_async_copy(src, dst, r.in_sem.at[len(loads)])
        loads[name].start()

    load("gw", r.gw_hbm, r.raw.at[0])
    load("uw", r.uw_hbm, r.raw.at[1])
    for name in ("ld", "q", "k", "v"):
        load(name, getattr(r, name + "_hbm"), getattr(r, name))
    load("dw", r.dw_hbm, r.slab.at[2])
    for name in ("g", "hg", "ow", "mg"):
        load(name, getattr(r, name + "_hbm"), getattr(r, name))
    mine = pl.multiple_of(tp * quarter, quarter)
    load("res", r.res_hbm.at[pl.ds(mine, quarter)], r.res)

    def remote(src, dst, send, recv, peer):
        return pltpu.make_async_remote_copy(
            src_ref=src,
            dst_ref=dst,
            send_sem=send,
            recv_sem=recv,
            device_id=peer,
            device_id_type=MESH,
        )

    started = {}

    def go(build, guard=None):
        build().start()
        started.setdefault(guard, []).append(build)
        return build

    guards = {"c0": c == 0, "c1": c == 1, "up": jnp.logical_and(c == 1, z < nz - 1)}

    def piece(ref, m, zz):
        return ref.at[m, pl.ds(pl.multiple_of(zz * share, 16), share)]

    def slot(m, zz):
        return r.w2.at[zz] if m == 2 else r.wg.at[m, zz * XS + x]

    own_copies = {}

    def take_own(m):
        own_copies[m] = pltpu.make_async_copy(piece(r.slab, m, z), slot(m, z), r.own_sem.at[m])
        own_copies[m].start()

    for m, name in enumerate(("gw", "uw")):
        loads[name].wait()
        for j in range(r.raw.shape[2] // 128):
            r.slab[m, j * 128 : (j + 1) * 128, :] = jnp.transpose(
                r.raw[m, :, j * 128 : (j + 1) * 128]
            )
        take_own(m)
    loads["dw"].wait()
    take_own(2)
    pl.semaphore_wait(barrier, len(peers))

    def hand(m):
        return lambda: remote(
            r.slab.at[m], r.partner.at[m], r.h_send.at[m], r.h_recv.at[m], c_peer
        )

    def weight(m, e, k):
        source = r.partner if k else r.slab
        return lambda: remote(
            piece(source, m, zat[e]),
            slot(m, z),
            r.w_send.at[k, m, e],
            r.w_recv.at[m, e],
            dev(zat[e], x, y, k),
        )

    started["c0"] = [
        weight(m, e, k) for m in range(3) for e in range(1, nz) for k in range(CS)
    ]
    outer = jnp.logical_or(z == 0, z == nz - 1)
    outer_plan = ((0, 1), (1, 1), (0, 2), (0, 3), (2, 1), (1, 2), (1, 3))
    inner_head = ((0, 3), (0, 1), (1, 3), (1, 1))
    inner_tail = ((0, 2), (2, 1), (1, 2))

    def send_weights(plan, which=range(CS)):
        for m, e in plan:
            for k in which:
                weight(m, e, k)().start()

    def got_weight(m, e):
        weight(m, e, 0)().wait_recv()

    def forward(m, e):
        at = slot(m, zat[e])
        source = piece(r.slab, m, z) if e == 0 else at
        return lambda: remote(source, at, r.f_send.at[m, e], r.f_recv.at[m, e], x_peer)

    def pass_on(m, e):
        if e:
            got_weight(m, e)
        go(forward(m, e))

    @pl.when(c == 1)
    def _():
        for m in range(3):
            go(hand(m), "c1")

    @pl.when(jnp.logical_and(c == 0, jnp.logical_not(outer)))
    def _():
        send_weights(inner_head, (0,))

    for name in ("ld", "q", "k", "v"):
        loads[name].wait()
    ti = lax.broadcasted_iota(jnp.int32, (rows, rows), 0)
    si = lax.broadcasted_iota(jnp.int32, (rows, rows), 1)
    lower = si <= ti
    cumul = lax.dot_general(
        r.ld[...],
        (ti <= si).astype(F32),
        (((1,), (0,)), ((), ())),
        precision=lax.Precision.HIGHEST,
        preferred_element_type=F32,
    )
    half = hd // 2
    lane = lax.broadcasted_iota(jnp.int32, (1, hd), 1)
    low_half = lane < half
    index = jnp.where(low_half, lane, lane - half).astype(F32)
    freq = jnp.exp(index * (-math.log(10000.0) / (half - 1)))
    angles = (sp * rows + lax.broadcasted_iota(jnp.int32, (rows, hd), 0)).astype(F32) * freq
    cos = jnp.cos(angles)
    sin = jnp.sin(angles)
    sin = jnp.where(low_half, -sin, sin)
    for h in range(heads):
        cols = slice(h * hd, (h + 1) * hd)
        qf = r.q[:, cols].astype(F32)
        kf = r.k[:, cols].astype(F32)
        vb = r.v[:, cols]
        qb = (qf * cos + pltpu.roll(qf, half, 1) * sin).astype(BF16)
        kb = ((kf * cos + pltpu.roll(kf, half, 1) * sin) * hd ** (-0.5)).astype(BF16)
        along = jnp.broadcast_to(cumul[h : h + 1, :], (rows, rows))
        cum = jnp.transpose(along)
        spread = cum - along
        weight_ts = jnp.where(lower, jnp.exp(jnp.where(lower, spread, 0.0)), 0.0)
        probs = (dot_nt(qb, kb) * weight_ts).astype(BF16)
        r.inner[:, cols] = dot_nn(probs, vb)
        last = cum[rows - 1 :, :]
        kw = kb.astype(F32) * jnp.exp(last - cum)
        r.c_out[h] = dot_nn(jnp.transpose(kw).astype(BF16), vb).astype(BF16)
        r.t_out[h] = jnp.broadcast_to(jnp.exp(last), r.t_out.shape[1:])
        r.qrot[:, cols] = qb
        r.cumx[:, cols] = jnp.exp(cum)

    my_h, its_h = pl.ds(x * hh, hh), pl.ds((1 - x) * hh, hh)
    x_one, c_one = dev(z, 1 - x, y, 1), dev(z, x, y, 1)

    def cross_c(k):
        return lambda: remote(
            r.c_out.at[its_h], r.ci.at[1, k], r.cx_send.at[0], r.cx_recv.at[0, k], x_one
        )

    def cross_t(k):
        return lambda: remote(
            r.t_out.at[its_h], r.ti.at[1, k], r.cx_send.at[1], r.cx_recv.at[1, k], x_one
        )

    go(cross_c(c))
    go(cross_t(c))

    def near_c():
        return remote(r.c_out.at[my_h], r.ci.at[0, 0], r.cc_send.at[0], r.cc_recv.at[0], c_one)

    def near_t():
        return remote(r.t_out.at[my_h], r.ti.at[0, 0], r.cc_send.at[1], r.cc_recv.at[1], c_one)

    def chain():
        up = jnp.minimum(z + 1, nz - 1)
        return remote(r.ch_out, r.ch_in, r.ch_send, r.ch_recv, dev(up, x, y, 1))

    def state_x(k):
        return lambda: remote(
            r.so.at[1, k], r.s_in.at[1], r.so_send.at[k], r.s_recv.at[1], dev(z, 1 - x, y, k)
        )

    def state_c():
        return remote(
            r.so.at[0, 0], r.s_in.at[0], r.so_send.at[2], r.s_recv.at[0], dev(z, x, y, 0)
        )

    @pl.when(c == 0)
    def _():
        go(near_c, "c0")
        go(near_t, "c0")
        for m in range(3):
            hand(m)().wait_recv()

        @pl.when(outer)
        def _():
            send_weights(outer_plan)

        @pl.when(jnp.logical_not(outer))
        def _():
            send_weights(inner_head, (1,))
            send_weights(inner_tail)

    pass_on(0, 0)
    pass_on(1, 0)
    first = x == 0

    @pl.when(c == 1)
    def _():
        r.ci[0, 1] = r.c_out[my_h]
        r.ti[0, 1] = r.t_out[my_h]
        near_c().wait_recv()
        near_t().wait_recv()
        for k in range(CS):
            cross_c(k)().wait_recv()
            cross_t(k)().wait_recv()
        for k in range(CS):
            for i in range(hh):
                own_c, own_t = r.ci[0, k, i].astype(F32), r.ti[0, k, i][:1]
                other_c, other_t = r.ci[1, k, i].astype(F32), r.ti[1, k, i][:1]
                early_c = jnp.where(first, own_c, other_c)
                late_c = jnp.where(first, other_c, own_c)
                late_t = jnp.where(first, other_t, own_t)
                r.plane[k, i] = late_t * early_c + late_c

        @pl.when(z == 0)
        def _():
            r.ch_in[...] = jnp.zeros(r.ch_in.shape, BF16)

        @pl.when(z > 0)
        def _():
            chain().wait_recv()

        for k in range(CS):
            for i in range(hh):
                both_t = r.ti[0, k, i][:1] * r.ti[1, k, i][:1]
                state = r.ch_in[k, i].astype(F32)
                r.ch_out[k, i] = (both_t * state + r.plane[k, i]).astype(BF16)

        @pl.when(z < nz - 1)
        def _():
            go(chain, "up")

        for k in range(CS):
            for i in range(hh):
                early_c = jnp.where(first, r.ci[0, k, i], r.ci[1, k, i]).astype(F32)
                early_t = jnp.where(first, r.ti[0, k, i][:1], r.ti[1, k, i][:1])
                state = r.ch_in[k, i].astype(F32)
                after = early_t * state + early_c
                r.so[0, k, i] = jnp.where(first, state, after).astype(BF16)
                r.so[1, k, i] = jnp.where(first, after, state).astype(BF16)
        for k in range(CS):
            go(state_x(k), "c1")
        go(state_c, "c1")
        r.s_in[0] = r.so[0, 1]

    @pl.when(c == 0)
    def _():
        state_c().wait_recv()

    state_x(0)().wait_recv()
    loads["g"].wait()
    loads["hg"].wait()
    for h in range(heads):
        cols = slice(h * hd, (h + 1) * hd)
        state = r.s_in[lax.rem(x + h // hh, XS), h % hh]
        ret = r.inner[:, cols] + r.cumx[:, cols] * dot_nn(r.qrot[:, cols], state)
        scale = lax.rsqrt(jnp.mean(ret * ret, axis=-1, keepdims=True) + EPS)
        gf = r.g[:, cols].astype(F32)
        r.retained[:, cols] = (
            ret * scale * r.hg[:, cols] * (gf / (1.0 + jnp.exp(-gf)))
        ).astype(BF16)
    loads["ow"].wait()

    def mix_c():
        return remote(r.mc_out, r.mc_in, r.mix_send.at[0], r.mix_recv.at[0], c_peer)

    def mix_y():
        return remote(
            r.my_out, r.my_in, r.mix_send.at[1], r.mix_recv.at[1], dev(z, x, 1 - y, c)
        )

    def mix_part(cc):
        picked = [
            r.retained[pl.ds(pl.multiple_of((yy * CS + cc) * quarter, quarter), quarter), :]
            for yy in range(nt // CS)
        ]
        part = dot_nn(jnp.concatenate(picked, axis=0), r.ow[...])
        return part.reshape(nt // CS, quarter, part.shape[1])

    r.mc_out[...] = mix_part(1 - c).astype(BF16)
    go(mix_c)
    r.mix_own[...] = mix_part(c)
    mix_c().wait_recv()
    r.my_out[...] = (r.mix_own[1 - y] + r.mc_in[1 - y].astype(F32)).astype(BF16)
    go(mix_y)
    pass_on(0, 1)
    mixed = r.mix_own[y] + r.mc_in[y].astype(F32)
    mix_y().wait_recv()
    mixed += r.my_in[...].astype(F32)
    loads["res"].wait()
    loads["mg"].wait()
    mid = (r.res[...].astype(F32) + mixed).astype(BF16).astype(F32)
    for g in range(nz):
        for u in range(XS):
            at = g * group + u * width
            r.acc[g, u] = mid[:, at : at + width]
    r.normed[z, tp] = (
        mid * lax.rsqrt(jnp.mean(mid * mid, axis=-1, keepdims=True) + EPS) * r.mg[...]
    ).astype(BF16)

    def rows_c():
        rows_at = r.normed.at[z, tp]
        return remote(rows_at, rows_at, r.nc_send, r.nc_recv, c_peer)

    def pair(zz, yy):
        return r.normed.at[zz, pl.ds(yy * CS, CS)]

    def rows_z(k):
        to = zat[2] if k == 0 else zat[1]
        zz = zat[2] if k == 2 else z
        return lambda: remote(
            pair(zz, y), pair(zz, y), r.nz_send.at[k], r.nz_recv.at[k], dev(to, x, y, 1)
        )

    def rows_y(e):
        return lambda: remote(
            pair(zat[e], y),
            pair(zat[e], y),
            r.ny_send.at[e],
            r.ny_recv.at[e],
            dev(z, x, 1 - y, 1),
        )

    def rows_d(e, v):
        def build():
            rows_at = pair(zat[e], 1 - y if v else y)
            return remote(
                rows_at, rows_at, r.nd_send.at[v, e], r.nd_recv.at[v, e], dev(z, x, y, 0)
            )

        return build

    go(rows_c)
    rows_c().wait_recv()

    @pl.when(c == 1)
    def _():
        for k in range(2):
            go(rows_z(k), "c1")
        go(rows_y(0), "c1")

    pass_on(1, 1)
    pass_on(0, 2)

    @pl.when(c == 1)
    def _():
        rows_z(1)().wait_recv()
        go(rows_y(1), "c1")
        go(rows_d(1, 0), "c1")
        rows_y(0)().wait_recv()
        go(rows_d(0, 1), "c1")
        rows_z(0)().wait_recv()
        go(rows_z(2), "c1")
        go(rows_y(2), "c1")
        go(rows_d(2, 0), "c1")

    pass_on(0, 3)
    pass_on(1, 3)

    def send_down(if_outer, if_inner):
        @pl.when(outer)
        def _():
            send_weights(((2, if_outer),))

        @pl.when(jnp.logical_not(outer))
        def _():
            send_weights(((2, if_inner),))

    @pl.when(c == 1)
    def _():
        rows_y(1)().wait_recv()
        go(rows_d(1, 1), "c1")
        rows_z(2)().wait_recv()
        go(rows_y(3), "c1")
        go(rows_d(3, 0), "c1")
        rows_y(2)().wait_recv()
        go(rows_d(2, 1), "c1")
        rows_y(3)().wait_recv()
        go(rows_d(3, 1), "c1")

    @pl.when(c == 0)
    def _():
        rows_d(2, 0)().wait_recv()
        send_down(2, 3)

    pass_on(1, 2)

    @pl.when(c == 0)
    def _():
        rows_d(3, 0)().wait_recv()
        send_down(3, 2)
        rows_d(1, 0)().wait_recv()
        for e in range(nz):
            rows_d(e, 1)().wait_recv()

    def project(m, lo, hi):
        block = r.normed[lo:hi].reshape((hi - lo) * rows, r.normed.shape[3])
        total = dot_nt(block[:, :width], r.wg[m, 0])
        for s in range(1, ns):
            total += dot_nt(block[:, s * width : (s + 1) * width], r.wg[m, s])
        return total

    def hand_hidden(i):
        at = pl.ds(i * 2 * rows, 2 * rows)
        return lambda: remote(
            r.hidden.at[0, at], r.hidden.at[1, at], r.hx_send.at[i], r.hx_recv.at[i], x_peer
        )

    own_copies[0].wait()
    for e in range(nz):
        forward(0, e)().wait_recv()
    for i in range(nz // 2):
        gate = project(0, 2 * i, 2 * i + 2)
        r.gated[i] = gate / (1.0 + jnp.exp(-gate))
    own_copies[1].wait()
    for e in range(nz):
        forward(1, e)().wait_recv()
    for i in range(nz // 2):
        at = slice(i * 2 * rows, (i + 1) * 2 * rows)
        r.hidden[0, at, :] = (r.gated[i] * project(1, 2 * i, 2 * i + 2)).astype(BF16)
        go(hand_hidden(i))
    own_copies[2].wait()

    low = c == 0

    def t1(b, u):
        return lambda: remote(
            r.s1.at[b, u], r.r1.at[b, u], r.t1_send.at[b, u], r.t1_recv.at[b, u], c_peer
        )

    def t2(b, u, k):
        to = (dev(z, x, 1 - y, c), dev(zat[1], x, y, c), dev(zat[1], x, 1 - y, c))[k]
        there = b ^ 1 if k else b
        return lambda: remote(
            r.s2.at[b, u, k],
            r.r2.at[there, u, k],
            r.t2_send.at[b, u, k],
            r.t2_recv.at[there, u, k],
            to,
        )

    def t3(b, k):
        to = (dev(zat[2], x, y, c), dev(z, 1 - x, y, c), dev(zat[2], 1 - x, y, c))[k]
        return lambda: remote(
            r.s3.at[b, k], r.r3.at[b, k], r.t3_send.at[b, k], r.t3_recv.at[b, k], to
        )

    def compute(b, u):
        part = dot_nn(r.hidden[u], r.w2[zat[b]])
        for zz in range(nz):
            for yy in range(nt // CS):
                at = zz * rows + yy * CS * quarter
                even = part[at : at + quarter]
                odd = part[at + quarter : at + 2 * quarter]
                r.keep[b, u, yy, zz] = jnp.where(low, even, odd)
                r.s1[b, u, yy, zz] = jnp.where(low, odd, even).astype(BF16)
        go(t1(b, u))

    def second(b, u):
        t1(b, u)().wait_recv()

        def value(yy, e):
            return r.keep[b, u, yy, zat[e]] + r.r1[b, u, yy, zat[e]].astype(F32)

        for k, (yy, off) in enumerate(((1 - y, 0), (y, 1), (1 - y, 1))):
            for j in range(2):
                r.s2[b, u, k, j] = value(yy, off ^ (2 * j)).astype(BF16)
            go(t2(b, u, k))
        for e in (0, 2):
            r.keep[b, u, y, zat[e]] = value(y, e)

    def third(b, u):
        for k in range(3):
            t2(b ^ 1 if k else b, u, k)().wait_recv()

        def value(j):
            total = r.keep[b, u, y, zat[2 * j]]
            for k in range(3):
                total += r.r2[b, u, k, j].astype(F32)
            return total

        if u:
            for j in (1, 0):
                r.s3[b, 1 + j] = value(j).astype(BF16)
                go(t3(b, 1 + j))
        else:
            r.s3[b, 0] = value(1).astype(BF16)
            go(t3(b, 0))
            r.acc[zat[b], x] = r.acc[zat[b], x] + value(0)

    def last(b, k):
        t3(b, k)().wait_recv()
        g, v = zat[b if k == 1 else b ^ 2], x if k == 0 else 1 - x
        r.acc[g, v] = r.acc[g, v] + r.r3[b, k].astype(F32)

    def other_hidden():
        for i in range(nz // 2):
            hand_hidden(i)().wait_recv()

    compute(0, 0)
    got_weight(2, 1)
    compute(1, 0)
    second(0, 0)
    second(1, 0)
    got_weight(2, 3)
    compute(3, 0)
    third(0, 0)
    third(1, 0)
    second(3, 0)
    other_hidden()
    compute(0, 1)
    compute(1, 1)
    second(0, 1)
    compute(3, 1)
    second(1, 1)
    got_weight(2, 2)
    compute(2, 0)
    compute(2, 1)
    second(3, 1)
    second(2, 0)
    second(2, 1)
    third(0, 1)
    third(1, 1)
    for b in range(2):
        for k in range(3):
            last(b, k)
    for u in range(XS):
        third(3, u)
        third(2, u)
    for b in range(2, nz):
        for k in range(3):
            last(b, k)
    for g in range(nz):
        for u in range(XS):
            at = g * group + u * width
            r.out[:, at : at + width] = r.acc[g, u].astype(BF16)

    for guard, builds in started.items():

        def drain(builds=builds):
            for build in builds:
                build().wait_send()

        if guard is None:
            drain()
        else:
            pl.when(guards[guard])(drain)


def fast_body(
    queries,
    key_rows,
    value_rows,
    gate_input,
    log_decay,
    head_gain,
    out_weight,
    residual,
    mlp_gain,
    gate_weight,
    up_weight,
    down_weight,
):
    rows, wide = queries.shape
    heads = log_decay.shape[1]
    hd = wide // heads
    model = residual.shape[1]
    ns, nt = lax.axis_size("sp"), lax.axis_size("tp")
    nz = ns // XS
    quarter = rows // nt
    width, units = gate_weight.shape
    share = units // nz
    hh = heads // XS
    vmem = pltpu.VMEM
    dma = pltpu.SemaphoreType.DMA
    operands = {
        "q_hbm": queries,
        "k_hbm": key_rows,
        "v_hbm": value_rows,
        "g_hbm": gate_input,
        "ld_hbm": log_decay.T,
        "hg_hbm": head_gain.reshape(1, wide),
        "res_hbm": residual,
        "mg_hbm": mlp_gain.reshape(1, model),
        "ow_hbm": out_weight,
        "gw_hbm": gate_weight,
        "uw_hbm": up_weight,
        "dw_hbm": down_weight,
    }
    scratch = {
        "q": vmem((rows, wide), BF16),
        "k": vmem((rows, wide), BF16),
        "v": vmem((rows, wide), BF16),
        "g": vmem((rows, wide), BF16),
        "ld": vmem((heads, rows), F32),
        "hg": vmem((1, wide), F32),
        "res": vmem((quarter, model), BF16),
        "mg": vmem((1, model), F32),
        "ow": vmem(out_weight.shape, BF16),
        "raw": vmem((2, width, units), BF16),
        "slab": vmem((3, units, width), BF16),
        "partner": vmem((3, units, width), BF16),
        "wg": vmem((2, ns, share, width), BF16),
        "w2": vmem((nz, share, width), BF16),
        "qrot": vmem((rows, wide), BF16),
        "inner": vmem((rows, wide), F32),
        "cumx": vmem((rows, wide), F32),
        "c_out": vmem((heads, hd, hd), BF16),
        "t_out": vmem((heads, 8, hd), F32),
        "ci": vmem((XS, CS, hh, hd, hd), BF16),
        "ti": vmem((XS, CS, hh, 8, hd), F32),
        "plane": vmem((CS, hh, hd, hd), F32),
        "ch_in": vmem((CS, hh, hd, hd), BF16),
        "ch_out": vmem((CS, hh, hd, hd), BF16),
        "so": vmem((XS, CS, hh, hd, hd), BF16),
        "s_in": vmem((XS, hh, hd, hd), BF16),
        "retained": vmem((rows, wide), BF16),
        "mc_out": vmem((nt // CS, quarter, model), BF16),
        "mc_in": vmem((nt // CS, quarter, model), BF16),
        "mix_own": vmem((nt // CS, quarter, model), F32),
        "my_out": vmem((quarter, model), BF16),
        "my_in": vmem((quarter, model), BF16),
        "acc": vmem((nz, XS, quarter, width), F32),
        "normed": vmem((nz, nt, quarter, model), BF16),
        "gated": vmem((nz // 2, 2 * rows, share), F32),
        "hidden": vmem((XS, nz * rows, share), BF16),
        "keep": vmem((nz, XS, nt // CS, nz, quarter, width), F32),
        "s1": vmem((nz, XS, nt // CS, nz, quarter, width), BF16),
        "r1": vmem((nz, XS, nt // CS, nz, quarter, width), BF16),
        "s2": vmem((nz, XS, 3, 2, quarter, width), BF16),
        "r2": vmem((nz, XS, 3, 2, quarter, width), BF16),
        "s3": vmem((nz, 3, quarter, width), BF16),
        "r3": vmem((nz, 3, quarter, width), BF16),
        "in_sem": dma((len(operands),)),
        "own_sem": dma((3,)),
        "h_send": dma((3,)),
        "h_recv": dma((3,)),
        "w_send": dma((CS, 3, nz)),
        "w_recv": dma((3, nz)),
        "f_send": dma((2, nz)),
        "f_recv": dma((2, nz)),
        "cx_send": dma((2,)),
        "cx_recv": dma((2, CS)),
        "cc_send": dma((2,)),
        "cc_recv": dma((2,)),
        "ch_send": dma,
        "ch_recv": dma,
        "so_send": dma((3,)),
        "s_recv": dma((XS,)),
        "mix_send": dma((2,)),
        "mix_recv": dma((2,)),
        "nc_send": dma,
        "nc_recv": dma,
        "nz_send": dma((3,)),
        "nz_recv": dma((3,)),
        "ny_send": dma((nz,)),
        "ny_recv": dma((nz,)),
        "nd_send": dma((2, nz)),
        "nd_recv": dma((2, nz)),
        "hx_send": dma((nz // 2,)),
        "hx_recv": dma((nz // 2,)),
        "t1_send": dma((nz, XS)),
        "t1_recv": dma((nz, XS)),
        "t2_send": dma((nz, XS, 3)),
        "t2_recv": dma((nz, XS, 3)),
        "t3_send": dma((nz, 3)),
        "t3_recv": dma((nz, 3)),
    }
    names = list(operands) + ["out"] + list(scratch)
    return pl.pallas_call(
        functools.partial(kernel, names, nz, nt),
        out_shape=pltpu.VMEM((quarter, model), BF16),
        in_specs=[pl.BlockSpec(memory_space=pl.ANY)] * len(operands),
        out_specs=pl.BlockSpec(memory_space=pltpu.VMEM),
        scratch_shapes=list(scratch.values()),
        compiler_params=pltpu.CompilerParams(
            collective_id=0, has_side_effects=True, vmem_limit_bytes=60 * 1024 * 1024
        ),
    )(*operands.values())


def fits(mesh, queries, log_decay, gate_weight):
    ns, nt = mesh.shape["sp"], mesh.shape["tp"]
    tokens, wide = queries.shape
    if ns % XS or ns // XS != 4 or nt != 2 * CS or tokens // ns != BLOCK:
        return False
    nz = ns // XS
    hidden = gate_weight.shape[1] // nt
    return (
        gate_weight.shape[0] // ns % 128 == 0
        and hidden % (16 * nz) == 0
        and wide // log_decay.shape[1] == 128
        and BLOCK % (16 * nt) == 0
        and hidden % 128 == 0
        and log_decay.shape[1] // nt % XS == 0
    )


def solution(mesh):
    def run(*args):
        good = fits(mesh, args[0], args[4], args[9])
        return jax.shard_map(
            fast_body if good else body,
            mesh=mesh,
            in_specs=(
                P("sp", "tp"),
                P("sp", "tp"),
                P("sp", "tp"),
                P("sp", "tp"),
                P("sp", "tp"),
                P("tp"),
                P("tp", None),
                P("sp", None),
                P(),
                P("sp", "tp"),
                P("sp", "tp"),
                P("tp", "sp"),
            ),
            out_specs=P(("sp", "tp"), None),
            check_vma=False,
        )(*args)

    return run
```

```python
import functools
import math
import types

import jax
import jax.numpy as jnp
from jax import lax
from jax.experimental import pallas as pl
from jax.experimental.pallas import tpu as pltpu
from jax.sharding import PartitionSpec as P

BLOCK = 128


EPS = 1e-06


def prefix_2(x, axis, join, neutral):
    place = lax.axis_index(axis)
    gathered = jax.tree.map(
        lambda a, kind: lax.all_gather(a.astype(kind), axis), x, (jnp.bfloat16, jnp.bfloat16)
    )
    state = jax.tree.map(lambda a, e: jnp.zeros_like(a) + jnp.asarray(e, a.dtype), x, neutral)

    def one(step, state):
        return join(
            state,
            jax.tree.map(
                lambda a, own: lax.dynamic_index_in_dim(a, step, 0, False).astype(own.dtype),
                gathered,
                x,
            ),
        )

    return lax.fori_loop(0, place, one, state)


def rotate(values_in, positions):
    half = values_in.shape[-1] // 2
    freq = 10000.0 ** (-jnp.linspace(0.0, 1.0, half, dtype=jnp.float32))
    angles = positions * freq
    angles = jnp.concatenate([angles, angles], axis=-1)
    first = values_in[..., :half]
    second = values_in[..., half:]
    turned = jnp.concatenate([-second, first], axis=-1)
    return values_in * jnp.cos(angles) + turned * jnp.sin(angles)


def row_norm(stream, gain):
    return stream * lax.rsqrt(jnp.mean(stream * stream, axis=-1, keepdims=True) + EPS) * gain


def join_states(earlier, later):
    return (earlier[0] * later[0], later[0][:, None, None] * earlier[1] + later[1])


def body(
    queries,
    key_rows,
    value_rows,
    gate_input,
    log_decay,
    head_gain,
    out_weight,
    residual,
    mlp_gain,
    gate_weight,
    up_weight,
    down_weight,
):
    tok_rows = queries.shape[0]
    heads_here = log_decay.shape[1]
    head_size = head_gain.shape[0] // heads_here
    quarter = tok_rows // lax.axis_size("tp")
    offset = lax.axis_index("sp") * tok_rows
    positions = (offset + lax.iota(jnp.int32, tok_rows)).astype(jnp.float32)[:, None, None]
    q_rot = rotate(
        queries.reshape(tok_rows, heads_here, head_size).astype(jnp.float32), positions
    ).astype(jnp.bfloat16)
    k_rot = (
        rotate(key_rows.reshape(tok_rows, heads_here, head_size).astype(jnp.float32), positions)
        * head_size ** (-0.5)
    ).astype(jnp.bfloat16)
    blocks = tok_rows // BLOCK
    q_blocks = q_rot.reshape(blocks, BLOCK, heads_here, head_size)
    k_blocks = k_rot.reshape(blocks, BLOCK, heads_here, head_size)
    v_blocks = value_rows.reshape(blocks, BLOCK, heads_here, head_size)
    cumul = jnp.cumsum(log_decay.reshape(blocks, BLOCK, heads_here), axis=1)
    by_head = cumul.transpose(0, 2, 1)
    lower = jnp.tril(jnp.ones((BLOCK, BLOCK), dtype=bool))
    spread = by_head[:, :, :, None] - by_head[:, :, None, :]
    weight = jnp.where(lower, jnp.exp(jnp.where(lower, spread, 0.0)), 0.0)
    scores = jnp.einsum("nthd,nshd->nhts", q_blocks, k_blocks, preferred_element_type=jnp.float32)
    probs = (scores * weight).astype(jnp.bfloat16)
    inner = jnp.einsum("nhts,nshe->nthe", probs, v_blocks, preferred_element_type=jnp.float32)
    k_weighted = (
        k_blocks.astype(jnp.float32) * jnp.exp(cumul[:, -1:, :] - cumul)[..., None]
    ).astype(jnp.bfloat16)
    contrib = jnp.einsum(
        "nshd,nshe->nhde", k_weighted, v_blocks, preferred_element_type=jnp.float32
    )
    totals = jnp.exp(cumul[:, -1, :])

    def advance(carry, items):
        state, prefix = carry
        factor, update = items
        return ((state * factor[:, None, None] + update, prefix * factor), (state, prefix))

    start_state = jnp.zeros((heads_here, head_size, head_size), jnp.float32)
    start_prefix = jnp.ones((heads_here,), jnp.float32)
    (dev_state, dev_total), (local_before, prefixes) = lax.scan(
        advance, (start_state, start_prefix), (totals, contrib)
    )
    _, incoming = prefix_2((dev_total, dev_state), "sp", join_states, (start_prefix, start_state))
    before = local_before + prefixes[:, :, None, None] * incoming[None]
    cross = jnp.einsum(
        "nthd,nhde->nthe", q_blocks.astype(jnp.float32), before, precision=lax.Precision.HIGHEST
    )
    cross = cross * jnp.exp(cumul)[..., None]
    result = (inner + cross).reshape(tok_rows, heads_here, head_size)
    result = row_norm(result, head_gain.reshape(heads_here, head_size)).reshape(
        tok_rows, heads_here * head_size
    )
    retained = (result * jax.nn.silu(gate_input.astype(jnp.float32))).astype(jnp.bfloat16)
    picked = retained
    mixed = lax.psum_scatter(
        jnp.dot(picked, out_weight, preferred_element_type=jnp.float32).astype(jnp.bfloat16),
        "tp",
        scatter_dimension=0,
        tiled=True,
    ).astype(jnp.float32)
    own_rows = lax.dynamic_slice_in_dim(residual, lax.axis_index("tp") * quarter, quarter, 0)
    rows_mid = (own_rows.astype(jnp.float32) + mixed).astype(jnp.bfloat16)
    own_normed = row_norm(rows_mid.astype(jnp.float32), mlp_gain).astype(jnp.bfloat16)
    normed = lax.all_gather(own_normed, "tp", axis=0, tiled=True)
    gate = jnp.dot(
        normed,
        lax.all_gather(gate_weight, "sp", axis=0, tiled=True),
        preferred_element_type=jnp.float32,
    )
    upvals = jnp.dot(
        normed,
        lax.all_gather(up_weight, "sp", axis=0, tiled=True),
        preferred_element_type=jnp.float32,
    )
    full_down = lax.all_gather(down_weight, "sp", axis=1, tiled=True)
    hidden = (jax.nn.silu(gate) * upvals).astype(jnp.bfloat16)
    picked = hidden
    ffn = lax.psum_scatter(
        jnp.dot(picked, full_down, preferred_element_type=jnp.float32).astype(jnp.bfloat16),
        "tp",
        scatter_dimension=0,
        tiled=True,
    ).astype(jnp.float32)
    return (rows_mid.astype(jnp.float32) + ffn).astype(jnp.bfloat16)


MESH = pl.DeviceIdType.MESH
XS = 2
CS = 2
F32 = jnp.float32
BF16 = jnp.bfloat16


def dot_nt(a, b):
    return lax.dot_general(a, b, (((1,), (1,)), ((), ())), preferred_element_type=F32)


def dot_nn(a, b):
    return lax.dot_general(a, b, (((1,), (0,)), ((), ())), preferred_element_type=F32)


def kernel(names, nz, nt, *refs):
    r = types.SimpleNamespace(**dict(zip(names, refs)))
    sp = lax.axis_index("sp")
    tp = lax.axis_index("tp")
    z, x = sp // XS, lax.rem(sp, XS)
    y, c = tp // CS, lax.rem(tp, CS)
    rows = r.q.shape[0]
    heads = r.ld.shape[0]
    hh = heads // XS
    hd = r.q.shape[1] // heads
    quarter = rows // nt
    share, width = r.wg.shape[2], r.wg.shape[3]
    group = XS * width
    ns = nz * XS
    zat = [z, z + 1 - 2 * lax.rem(z, 2), lax.rem(z + 2, nz), nz - 1 - z]

    def dev(zz, xx, yy, cc):
        return (zz * XS + xx, yy * CS + cc)

    x_peer = dev(z, 1 - x, y, c)
    c_peer = dev(z, x, y, 1 - c)

    barrier = pltpu.get_barrier_semaphore()
    peers = [dev(zat[e], x, y, k) for e in range(1, nz) for k in range(CS)]
    peers += [c_peer]
    peers += [dev(z, 1 - x, y, k) for k in range(CS)]
    peers += [dev(z, x, 1 - y, k) for k in range(CS)]
    for peer in peers:
        pl.semaphore_signal(barrier, inc=1, device_id=peer, device_id_type=MESH)

    loads = {}

    def load(name, src, dst):
        loads[name] = pltpu.make_async_copy(src, dst, r.in_sem.at[len(loads)])
        loads[name].start()

    load("gw", r.gw_hbm, r.raw.at[0])
    load("uw", r.uw_hbm, r.raw.at[1])
    for name in ("ld", "q", "k", "v"):
        load(name, getattr(r, name + "_hbm"), getattr(r, name))
    load("dw", r.dw_hbm, r.slab.at[2])
    for name in ("g", "hg", "ow", "mg"):
        load(name, getattr(r, name + "_hbm"), getattr(r, name))
    mine = pl.multiple_of(tp * quarter, quarter)
    load("res", r.res_hbm.at[pl.ds(mine, quarter)], r.res)

    def remote(src, dst, send, recv, peer):
        return pltpu.make_async_remote_copy(
            src_ref=src,
            dst_ref=dst,
            send_sem=send,
            recv_sem=recv,
            device_id=peer,
            device_id_type=MESH,
        )

    started = {}

    def go(build, guard=None):
        build().start()
        started.setdefault(guard, []).append(build)
        return build

    guards = {"c0": c == 0, "c1": c == 1, "up": jnp.logical_and(c == 1, z < nz - 1)}

    def piece(ref, m, zz):
        return ref.at[m, pl.ds(pl.multiple_of(zz * share, 16), share)]

    def slot(m, zz):
        return r.wg.at[m, zz * XS + x]

    own_copies = {}

    def take_own(m):
        own_copies[m] = pltpu.make_async_copy(piece(r.slab, m, z), slot(m, z), r.own_sem.at[m])
        own_copies[m].start()

    for m, name in enumerate(("gw", "uw")):
        loads[name].wait()
        for j in range(r.raw.shape[2] // 128):
            r.slab[m, j * 128 : (j + 1) * 128, :] = jnp.transpose(
                r.raw[m, :, j * 128 : (j + 1) * 128]
            )
        take_own(m)
    loads["dw"].wait()
    take_own(2)
    pl.semaphore_wait(barrier, len(peers))

    def hand(m):
        return lambda: remote(
            r.slab.at[m], r.partner.at[m], r.h_send.at[m], r.h_recv.at[m], c_peer
        )

    def weight(m, e, k):
        source = r.partner if k else r.slab
        return lambda: remote(
            piece(source, m, zat[e]),
            slot(m, z),
            r.w_send.at[k, m, e],
            r.w_recv.at[m, e],
            dev(zat[e], x, y, k),
        )

    started["c0"] = [
        weight(m, e, k) for m in range(3) for e in range(1, nz) for k in range(CS)
    ]
    outer = jnp.logical_or(z == 0, z == nz - 1)
    outer_head = ((0, 1), (1, 1))
    outer_tail = ((2, 1), (0, 2), (0, 3), (1, 2), (1, 3))
    inner_head = ((0, 3), (0, 1), (1, 3), (1, 1))
    inner_tail = ((0, 2), (2, 1), (1, 2))

    def send_weights(plan, which=range(CS)):
        for m, e in plan:
            for k in which:
                weight(m, e, k)().start()

    def got_weight(m, e):
        weight(m, e, 0)().wait_recv()

    def forward(m, e):
        at = slot(m, zat[e])
        source = piece(r.slab, m, z) if e == 0 else at
        return lambda: remote(source, at, r.f_send.at[m, e], r.f_recv.at[m, e], x_peer)

    def pass_on(m, e):
        if e:
            got_weight(m, e)
        go(forward(m, e))

    def pass_if(when, pieces):
        @pl.when(when)
        def _():
            for m, e in pieces:
                got_weight(m, e)
                forward(m, e)().start()

    near = ((0, 1), (1, 1))
    started[None] = [forward(m, e) for m, e in near + ((0, 3),)]

    @pl.when(c == 1)
    def _():
        for m in range(3):
            go(hand(m), "c1")

    @pl.when(jnp.logical_and(c == 0, outer))
    def _():
        send_weights(outer_head, (0,))

    @pl.when(jnp.logical_and(c == 0, jnp.logical_not(outer)))
    def _():
        send_weights(inner_head, (0,))

    for name in ("ld", "q", "k", "v"):
        loads[name].wait()
    ti = lax.broadcasted_iota(jnp.int32, (rows, rows), 0)
    si = lax.broadcasted_iota(jnp.int32, (rows, rows), 1)
    lower = si <= ti
    cumul = lax.dot_general(
        r.ld[...],
        (ti <= si).astype(F32),
        (((1,), (0,)), ((), ())),
        precision=lax.Precision.HIGHEST,
        preferred_element_type=F32,
    )
    half = hd // 2
    lane = lax.broadcasted_iota(jnp.int32, (1, hd), 1)
    low_half = lane < half
    index = jnp.where(low_half, lane, lane - half).astype(F32)
    freq = jnp.exp(index * (-math.log(10000.0) / (half - 1)))
    angles = (sp * rows + lax.broadcasted_iota(jnp.int32, (rows, hd), 0)).astype(F32) * freq
    cos = jnp.cos(angles)
    sin = jnp.sin(angles)
    sin = jnp.where(low_half, -sin, sin)
    for h in range(heads):
        cols = slice(h * hd, (h + 1) * hd)
        qf = r.q[:, cols].astype(F32)
        kf = r.k[:, cols].astype(F32)
        vb = r.v[:, cols]
        qb = (qf * cos + pltpu.roll(qf, half, 1) * sin).astype(BF16)
        kb = ((kf * cos + pltpu.roll(kf, half, 1) * sin) * hd ** (-0.5)).astype(BF16)
        along = jnp.broadcast_to(cumul[h : h + 1, :], (rows, rows))
        cum = jnp.transpose(along)
        spread = cum - along
        weight_ts = jnp.where(lower, jnp.exp(jnp.where(lower, spread, 0.0)), 0.0)
        probs = (dot_nt(qb, kb) * weight_ts).astype(BF16)
        r.inner[:, cols] = dot_nn(probs, vb)
        last = cum[rows - 1 :, :]
        kw = kb.astype(F32) * jnp.exp(last - cum)
        r.c_out[h] = dot_nn(jnp.transpose(kw).astype(BF16), vb).astype(BF16)
        r.t_out[h] = jnp.broadcast_to(jnp.exp(last), r.t_out.shape[1:])
        r.qrot[:, cols] = qb
        r.cumx[:, cols] = jnp.exp(cum)

    my_h, its_h = pl.ds(x * hh, hh), pl.ds((1 - x) * hh, hh)
    x_one, c_one = dev(z, 1 - x, y, 1), dev(z, x, y, 1)

    def cross_c(k):
        return lambda: remote(
            r.c_out.at[its_h], r.ci.at[1, k], r.cx_send.at[0], r.cx_recv.at[0, k], x_one
        )

    def cross_t(k):
        return lambda: remote(
            r.t_out.at[its_h], r.ti.at[1, k], r.cx_send.at[1], r.cx_recv.at[1, k], x_one
        )

    go(cross_c(c))
    go(cross_t(c))

    def near_c():
        return remote(r.c_out.at[my_h], r.ci.at[0, 0], r.cc_send.at[0], r.cc_recv.at[0], c_one)

    def near_t():
        return remote(r.t_out.at[my_h], r.ti.at[0, 0], r.cc_send.at[1], r.cc_recv.at[1], c_one)

    def chain():
        up = jnp.minimum(z + 1, nz - 1)
        return remote(r.ch_out, r.ch_in, r.ch_send, r.ch_recv, dev(up, x, y, 1))

    def state_x(k):
        return lambda: remote(
            r.so.at[1, k], r.s_in.at[1], r.so_send.at[k], r.s_recv.at[1], dev(z, 1 - x, y, k)
        )

    def state_c():
        return remote(
            r.so.at[0, 0], r.s_in.at[0], r.so_send.at[2], r.s_recv.at[0], dev(z, x, y, 0)
        )

    @pl.when(c == 0)
    def _():
        go(near_c, "c0")
        go(near_t, "c0")
        for m in range(3):
            hand(m)().wait_recv()

        @pl.when(outer)
        def _():
            send_weights(outer_head, (1,))
            send_weights(outer_tail)

        @pl.when(jnp.logical_not(outer))
        def _():
            send_weights(inner_head, (1,))
            send_weights(inner_tail)

    pass_on(0, 0)
    pass_on(1, 0)
    first = x == 0
    late = z >= nz // 2

    @pl.when(c == 1)
    def _():
        r.ci[0, 1] = r.c_out[my_h]
        r.ti[0, 1] = r.t_out[my_h]
        near_c().wait_recv()
        near_t().wait_recv()
        for k in range(CS):
            cross_c(k)().wait_recv()
            cross_t(k)().wait_recv()
        for k in range(CS):
            for i in range(hh):
                own_c, own_t = r.ci[0, k, i].astype(F32), r.ti[0, k, i][:1]
                other_c, other_t = r.ci[1, k, i].astype(F32), r.ti[1, k, i][:1]
                early_c = jnp.where(first, own_c, other_c)
                late_c = jnp.where(first, other_c, own_c)
                late_t = jnp.where(first, other_t, own_t)
                r.plane[k, i] = late_t * early_c + late_c

        pass_if(late, near)

        @pl.when(z == 0)
        def _():
            r.ch_in[...] = jnp.zeros(r.ch_in.shape, BF16)

        @pl.when(z > 0)
        def _():
            chain().wait_recv()

        for k in range(CS):
            for i in range(hh):
                both_t = r.ti[0, k, i][:1] * r.ti[1, k, i][:1]
                state = r.ch_in[k, i].astype(F32)
                r.ch_out[k, i] = (both_t * state + r.plane[k, i]).astype(BF16)

        @pl.when(z < nz - 1)
        def _():
            go(chain, "up")

        for k in range(CS):
            for i in range(hh):
                early_c = jnp.where(first, r.ci[0, k, i], r.ci[1, k, i]).astype(F32)
                early_t = jnp.where(first, r.ti[0, k, i][:1], r.ti[1, k, i][:1])
                state = r.ch_in[k, i].astype(F32)
                after = early_t * state + early_c
                r.so[0, k, i] = jnp.where(first, state, after).astype(BF16)
                r.so[1, k, i] = jnp.where(first, after, state).astype(BF16)
        for k in range(CS):
            go(state_x(k), "c1")
        go(state_c, "c1")
        r.s_in[0] = r.so[0, 1]

    @pl.when(c == 0)
    def _():
        pass_if(late, near)
        state_c().wait_recv()

    own_copies[2].wait()
    pass_on(2, 0)
    state_x(0)().wait_recv()
    loads["g"].wait()
    loads["hg"].wait()
    for h in range(heads):
        cols = slice(h * hd, (h + 1) * hd)
        state = r.s_in[lax.rem(x + h // hh, XS), h % hh]
        ret = r.inner[:, cols] + r.cumx[:, cols] * dot_nn(r.qrot[:, cols], state)
        scale = lax.rsqrt(jnp.mean(ret * ret, axis=-1, keepdims=True) + EPS)
        gf = r.g[:, cols].astype(F32)
        r.retained[:, cols] = (
            ret * scale * r.hg[:, cols] * (gf / (1.0 + jnp.exp(-gf)))
        ).astype(BF16)
    loads["ow"].wait()

    def mix_c():
        return remote(r.mc_out, r.mc_in, r.mix_send.at[0], r.mix_recv.at[0], c_peer)

    def mix_y():
        return remote(
            r.my_out, r.my_in, r.mix_send.at[1], r.mix_recv.at[1], dev(z, x, 1 - y, c)
        )

    def mix_part(cc):
        picked = [
            r.retained[pl.ds(pl.multiple_of((yy * CS + cc) * quarter, quarter), quarter), :]
            for yy in range(nt // CS)
        ]
        part = dot_nn(jnp.concatenate(picked, axis=0), r.ow[...])
        return part.reshape(nt // CS, quarter, part.shape[1])

    r.mc_out[...] = mix_part(1 - c).astype(BF16)
    go(mix_c)
    r.mix_own[...] = mix_part(c)
    mix_c().wait_recv()
    r.my_out[...] = (r.mix_own[1 - y] + r.mc_in[1 - y].astype(F32)).astype(BF16)
    go(mix_y)
    early = jnp.logical_not(late)
    pass_if(early, near)
    pass_on(0, 2)
    pass_if(late, ((0, 3),))
    mixed = r.mix_own[y] + r.mc_in[y].astype(F32)
    mix_y().wait_recv()
    mixed += r.my_in[...].astype(F32)
    loads["res"].wait()
    loads["mg"].wait()
    mid = (r.res[...].astype(F32) + mixed).astype(BF16).astype(F32)
    for g in range(nz):
        for u in range(XS):
            at = g * group + u * width
            r.acc[g, u] = mid[:, at : at + width]
    r.normed[z, tp] = (
        mid * lax.rsqrt(jnp.mean(mid * mid, axis=-1, keepdims=True) + EPS) * r.mg[...]
    ).astype(BF16)

    def rows_c():
        rows_at = r.normed.at[z, tp]
        return remote(rows_at, rows_at, r.nc_send, r.nc_recv, c_peer)

    def rows_of(zz, yy, j):
        return r.normed.at[zz, yy * CS + j]

    def rows_z(k, j):
        to = zat[2] if k == 0 else zat[1]
        zz = zat[2] if k == 2 else z
        return lambda: remote(
            rows_of(zz, y, j),
            rows_of(zz, y, j),
            r.nz_send.at[k, j],
            r.nz_recv.at[k, j],
            dev(to, x, y, 1),
        )

    def rows_y(e, j):
        return lambda: remote(
            rows_of(zat[e], y, j),
            rows_of(zat[e], y, j),
            r.ny_send.at[e, j],
            r.ny_recv.at[e, j],
            dev(z, x, 1 - y, 1),
        )

    def rows_d(e, v, j):
        def build():
            rows_at = rows_of(zat[e], 1 - y if v else y, j)
            return remote(
                rows_at, rows_at, r.nd_send.at[v, e, j], r.nd_recv.at[v, e, j], dev(z, x, y, 0)
            )

        return build

    go(rows_c)

    def send_down(if_outer, if_inner):
        @pl.when(outer)
        def _():
            send_weights(((2, if_outer),))

        @pl.when(jnp.logical_not(outer))
        def _():
            send_weights(((2, if_inner),))

    @pl.when(c == 1)
    def _():
        for j in (1, 0):
            if j == 0:
                rows_c().wait_recv()
            for k in range(2):
                go(rows_z(k, j), "c1")
            go(rows_y(0, j), "c1")

    @pl.when(c == 0)
    def _():
        rows_c().wait_recv()

    pass_if(early, ((0, 3),))
    pass_on(2, 1)
    pass_on(1, 3)

    @pl.when(c == 1)
    def _():
        for j in (1, 0):
            rows_z(1, j)().wait_recv()
            go(rows_y(1, j), "c1")
            go(rows_d(1, 0, j), "c1")
        for j in (1, 0):
            rows_y(0, j)().wait_recv()
            go(rows_d(0, 1, j), "c1")
        for j in (1, 0):
            rows_z(0, j)().wait_recv()
            go(rows_z(2, j), "c1")
            go(rows_y(2, j), "c1")
            go(rows_d(2, 0, j), "c1")

    pass_on(1, 2)

    @pl.when(c == 0)
    def _():
        for j in (1, 0):
            rows_d(2, 0, j)().wait_recv()
        send_down(2, 3)

    @pl.when(c == 1)
    def _():
        for j in (1, 0):
            rows_y(1, j)().wait_recv()
            go(rows_d(1, 1, j), "c1")
        for j in (1, 0):
            rows_z(2, j)().wait_recv()
            go(rows_y(3, j), "c1")
            go(rows_d(3, 0, j), "c1")

    @pl.when(c == 0)
    def _():
        for j in (1, 0):
            rows_d(3, 0, j)().wait_recv()
        send_down(3, 2)
        for e, v in ((1, 0), (0, 1), (1, 1)):
            for j in (1, 0):
                rows_d(e, v, j)().wait_recv()

    def project(m, half_z):
        block = r.normed[pl.ds(2 * half_z, 2)].reshape(2 * rows, r.normed.shape[3])
        total = dot_nt(block[:, :width], r.wg[m, 0])
        for s in range(1, ns):
            total += dot_nt(block[:, s * width : (s + 1) * width], r.wg[m, s])
        return total

    def gate_rows(half_z):
        gate = project(0, half_z)
        r.gated[half_z] = gate / (1.0 + jnp.exp(-gate))

    def up_rows(half_z):
        at = pl.ds(pl.multiple_of(half_z * 2 * rows, 2 * rows), 2 * rows)
        r.hidden[at, :] = (r.gated[half_z] * project(1, half_z)).astype(BF16)

    own_half = z // 2
    own_copies[0].wait()
    for e in range(nz):
        forward(0, e)().wait_recv()
    gate_rows(own_half)

    @pl.when(c == 1)
    def _():
        for e in (2, 3):
            for j in (1, 0):
                rows_y(e, j)().wait_recv()
                go(rows_d(e, 1, j), "c1")

    own_copies[1].wait()
    for e in range(nz):
        forward(1, e)().wait_recv()
    up_rows(own_half)

    @pl.when(c == 0)
    def _():
        for e in (2, 3):
            for j in (1, 0):
                rows_d(e, 1, j)().wait_recv()

    gate_rows(1 - own_half)
    up_rows(1 - own_half)

    low = c == 0

    def t1(b, u):
        return lambda: remote(
            r.s1.at[b, u], r.r1.at[b, u], r.t1_send.at[b, u], r.t1_recv.at[b, u], c_peer
        )

    def t2(b, u):
        return lambda: remote(
            r.s2.at[b, u],
            r.r2.at[b, u],
            r.t2_send.at[b, u],
            r.t2_recv.at[b, u],
            dev(z, x, 1 - y, c),
        )

    def t3(b, u, e):
        return lambda: remote(
            r.s3.at[b, u, e],
            r.r3.at[b, u, e],
            r.t3_send.at[b, u, e],
            r.t3_recv.at[b, u, e],
            dev(zat[e], x, y, c),
        )

    def side(u):
        return 1 - x if u else x

    def compute(b, u):
        if u:
            forward(2, b)().wait_recv()
        part = dot_nn(r.hidden[...], r.wg[2, zat[b] * XS + side(u)])
        for zz in range(nz):
            for yy in range(nt // CS):
                at = zz * rows + yy * CS * quarter
                even = part[at : at + quarter]
                odd = part[at + quarter : at + 2 * quarter]
                r.keep[b, u, yy, zz] = jnp.where(low, even, odd)
                r.s1[b, u, yy, zz] = jnp.where(low, odd, even).astype(BF16)
        go(t1(b, u))

    def second(b, u):
        t1(b, u)().wait_recv()
        r.s2[b, u] = (r.keep[b, u, 1 - y] + r.r1[b, u, 1 - y].astype(F32)).astype(BF16)
        go(t2(b, u))
        r.keep[b, u, y] = r.keep[b, u, y] + r.r1[b, u, y].astype(F32)

    def third(b, u):
        t2(b, u)().wait_recv()
        for e in (3, 2, 1):
            total = r.keep[b, u, y, zat[e]] + r.r2[b, u, zat[e]].astype(F32)
            r.s3[b, u, e] = total.astype(BF16)
            go(t3(b, u, e))
        total = r.keep[b, u, y, z] + r.r2[b, u, z].astype(F32)
        r.acc[zat[b], side(u)] = r.acc[zat[b], side(u)] + total

    def last(b, u):
        for e in (1, 3, 2):
            t3(b, u, e)().wait_recv()
            g = zat[b ^ e]
            r.acc[g, side(u)] = r.acc[g, side(u)] + r.r3[b, u, e].astype(F32)

    for b in range(2):
        for u in range(XS):
            compute(b, u)
    for b in range(2):
        for u in range(XS):
            second(b, u)
    pass_on(2, 3)
    compute(3, 0)
    third(0, 0)
    third(0, 1)
    pass_on(2, 2)
    compute(2, 0)
    second(3, 0)
    third(1, 0)
    third(1, 1)
    second(2, 0)
    compute(3, 1)
    second(3, 1)
    compute(2, 1)
    second(2, 1)
    for b, u in ((3, 0), (2, 0), (3, 1), (2, 1)):
        third(b, u)
    for b in (0, 1):
        for u in range(XS):
            last(b, u)
    for b, u in ((3, 0), (2, 0), (3, 1), (2, 1)):
        last(b, u)
    for g in range(nz):
        for u in range(XS):
            at = g * group + u * width
            r.out[:, at : at + width] = r.acc[g, u].astype(BF16)

    for guard, builds in started.items():

        def drain(builds=builds):
            for build in builds:
                build().wait_send()

        if guard is None:
            drain()
        else:
            pl.when(guards[guard])(drain)


def fast_body(
    queries,
    key_rows,
    value_rows,
    gate_input,
    log_decay,
    head_gain,
    out_weight,
    residual,
    mlp_gain,
    gate_weight,
    up_weight,
    down_weight,
):
    rows, wide = queries.shape
    heads = log_decay.shape[1]
    hd = wide // heads
    model = residual.shape[1]
    ns, nt = lax.axis_size("sp"), lax.axis_size("tp")
    nz = ns // XS
    quarter = rows // nt
    width, units = gate_weight.shape
    share = units // nz
    hh = heads // XS
    vmem = pltpu.VMEM
    dma = pltpu.SemaphoreType.DMA
    operands = {
        "q_hbm": queries,
        "k_hbm": key_rows,
        "v_hbm": value_rows,
        "g_hbm": gate_input,
        "ld_hbm": log_decay.T,
        "hg_hbm": head_gain.reshape(1, wide),
        "res_hbm": residual,
        "mg_hbm": mlp_gain.reshape(1, model),
        "ow_hbm": out_weight,
        "gw_hbm": gate_weight,
        "uw_hbm": up_weight,
        "dw_hbm": down_weight,
    }
    scratch = {
        "q": vmem((rows, wide), BF16),
        "k": vmem((rows, wide), BF16),
        "v": vmem((rows, wide), BF16),
        "g": vmem((rows, wide), BF16),
        "ld": vmem((heads, rows), F32),
        "hg": vmem((1, wide), F32),
        "res": vmem((quarter, model), BF16),
        "mg": vmem((1, model), F32),
        "ow": vmem(out_weight.shape, BF16),
        "raw": vmem((2, width, units), BF16),
        "slab": vmem((3, units, width), BF16),
        "partner": vmem((3, units, width), BF16),
        "wg": vmem((3, ns, share, width), BF16),
        "qrot": vmem((rows, wide), BF16),
        "inner": vmem((rows, wide), F32),
        "cumx": vmem((rows, wide), F32),
        "c_out": vmem((heads, hd, hd), BF16),
        "t_out": vmem((heads, 8, hd), F32),
        "ci": vmem((XS, CS, hh, hd, hd), BF16),
        "ti": vmem((XS, CS, hh, 8, hd), F32),
        "plane": vmem((CS, hh, hd, hd), F32),
        "ch_in": vmem((CS, hh, hd, hd), BF16),
        "ch_out": vmem((CS, hh, hd, hd), BF16),
        "so": vmem((XS, CS, hh, hd, hd), BF16),
        "s_in": vmem((XS, hh, hd, hd), BF16),
        "retained": vmem((rows, wide), BF16),
        "mc_out": vmem((nt // CS, quarter, model), BF16),
        "mc_in": vmem((nt // CS, quarter, model), BF16),
        "mix_own": vmem((nt // CS, quarter, model), F32),
        "my_out": vmem((quarter, model), BF16),
        "my_in": vmem((quarter, model), BF16),
        "acc": vmem((nz, XS, quarter, width), F32),
        "normed": vmem((nz, nt, quarter, model), BF16),
        "gated": vmem((nz // 2, 2 * rows, share), F32),
        "hidden": vmem((nz * rows, share), BF16),
        "keep": vmem((nz, XS, nt // CS, nz, quarter, width), F32),
        "s1": vmem((nz, XS, nt // CS, nz, quarter, width), BF16),
        "r1": vmem((nz, XS, nt // CS, nz, quarter, width), BF16),
        "s2": vmem((nz, XS, nz, quarter, width), BF16),
        "r2": vmem((nz, XS, nz, quarter, width), BF16),
        "s3": vmem((nz, XS, nz, quarter, width), BF16),
        "r3": vmem((nz, XS, nz, quarter, width), BF16),
        "in_sem": dma((len(operands),)),
        "own_sem": dma((3,)),
        "h_send": dma((3,)),
        "h_recv": dma((3,)),
        "w_send": dma((CS, 3, nz)),
        "w_recv": dma((3, nz)),
        "f_send": dma((3, nz)),
        "f_recv": dma((3, nz)),
        "cx_send": dma((2,)),
        "cx_recv": dma((2, CS)),
        "cc_send": dma((2,)),
        "cc_recv": dma((2,)),
        "ch_send": dma,
        "ch_recv": dma,
        "so_send": dma((3,)),
        "s_recv": dma((XS,)),
        "mix_send": dma((2,)),
        "mix_recv": dma((2,)),
        "nc_send": dma,
        "nc_recv": dma,
        "nz_send": dma((3, CS)),
        "nz_recv": dma((3, CS)),
        "ny_send": dma((nz, CS)),
        "ny_recv": dma((nz, CS)),
        "nd_send": dma((2, nz, CS)),
        "nd_recv": dma((2, nz, CS)),
        "t1_send": dma((nz, XS)),
        "t1_recv": dma((nz, XS)),
        "t2_send": dma((nz, XS)),
        "t2_recv": dma((nz, XS)),
        "t3_send": dma((nz, XS, nz)),
        "t3_recv": dma((nz, XS, nz)),
    }
    names = list(operands) + ["out"] + list(scratch)
    return pl.pallas_call(
        functools.partial(kernel, names, nz, nt),
        out_shape=pltpu.VMEM((quarter, model), BF16),
        in_specs=[pl.BlockSpec(memory_space=pl.ANY)] * len(operands),
        out_specs=pl.BlockSpec(memory_space=pltpu.VMEM),
        scratch_shapes=list(scratch.values()),
        compiler_params=pltpu.CompilerParams(
            collective_id=0, has_side_effects=True, vmem_limit_bytes=60 * 1024 * 1024
        ),
    )(*operands.values())


def fits(mesh, queries, log_decay, gate_weight):
    ns, nt = mesh.shape["sp"], mesh.shape["tp"]
    tokens, wide = queries.shape
    if ns % XS or ns // XS != 4 or nt != 2 * CS or tokens // ns != BLOCK:
        return False
    nz = ns // XS
    hidden = gate_weight.shape[1] // nt
    return (
        gate_weight.shape[0] // ns % 128 == 0
        and hidden % (16 * nz) == 0
        and wide // log_decay.shape[1] == 128
        and BLOCK % (16 * nt) == 0
        and hidden % 128 == 0
        and log_decay.shape[1] // nt % XS == 0
    )


def solution(mesh):
    def run(*args):
        good = fits(mesh, args[0], args[4], args[9])
        return jax.shard_map(
            fast_body if good else body,
            mesh=mesh,
            in_specs=(
                P("sp", "tp"),
                P("sp", "tp"),
                P("sp", "tp"),
                P("sp", "tp"),
                P("sp", "tp"),
                P("tp"),
                P("tp", None),
                P("sp", None),
                P(),
                P("sp", "tp"),
                P("sp", "tp"),
                P("tp", "sp"),
            ),
            out_specs=P(("sp", "tp"), None),
            check_vma=False,
        )(*args)

    return run
```

```python
import functools
import math
import types

import jax
import jax.numpy as jnp
from jax import lax
from jax.experimental import pallas as pl
from jax.experimental.pallas import tpu as pltpu
from jax.sharding import PartitionSpec as P

BLOCK = 128


EPS = 1e-06


def prefix_2(x, axis, join, neutral):
    place = lax.axis_index(axis)
    gathered = jax.tree.map(
        lambda a, kind: lax.all_gather(a.astype(kind), axis), x, (jnp.bfloat16, jnp.bfloat16)
    )
    state = jax.tree.map(lambda a, e: jnp.zeros_like(a) + jnp.asarray(e, a.dtype), x, neutral)

    def one(step, state):
        return join(
            state,
            jax.tree.map(
                lambda a, own: lax.dynamic_index_in_dim(a, step, 0, False).astype(own.dtype),
                gathered,
                x,
            ),
        )

    return lax.fori_loop(0, place, one, state)


def rotate(values_in, positions):
    half = values_in.shape[-1] // 2
    freq = 10000.0 ** (-jnp.linspace(0.0, 1.0, half, dtype=jnp.float32))
    angles = positions * freq
    angles = jnp.concatenate([angles, angles], axis=-1)
    first = values_in[..., :half]
    second = values_in[..., half:]
    turned = jnp.concatenate([-second, first], axis=-1)
    return values_in * jnp.cos(angles) + turned * jnp.sin(angles)


def row_norm(stream, gain):
    return stream * lax.rsqrt(jnp.mean(stream * stream, axis=-1, keepdims=True) + EPS) * gain


def join_states(earlier, later):
    return (earlier[0] * later[0], later[0][:, None, None] * earlier[1] + later[1])


def body(
    queries,
    key_rows,
    value_rows,
    gate_input,
    log_decay,
    head_gain,
    out_weight,
    residual,
    mlp_gain,
    gate_weight,
    up_weight,
    down_weight,
):
    tok_rows = queries.shape[0]
    heads_here = log_decay.shape[1]
    head_size = head_gain.shape[0] // heads_here
    quarter = tok_rows // lax.axis_size("tp")
    offset = lax.axis_index("sp") * tok_rows
    positions = (offset + lax.iota(jnp.int32, tok_rows)).astype(jnp.float32)[:, None, None]
    q_rot = rotate(
        queries.reshape(tok_rows, heads_here, head_size).astype(jnp.float32), positions
    ).astype(jnp.bfloat16)
    k_rot = (
        rotate(key_rows.reshape(tok_rows, heads_here, head_size).astype(jnp.float32), positions)
        * head_size ** (-0.5)
    ).astype(jnp.bfloat16)
    blocks = tok_rows // BLOCK
    q_blocks = q_rot.reshape(blocks, BLOCK, heads_here, head_size)
    k_blocks = k_rot.reshape(blocks, BLOCK, heads_here, head_size)
    v_blocks = value_rows.reshape(blocks, BLOCK, heads_here, head_size)
    cumul = jnp.cumsum(log_decay.reshape(blocks, BLOCK, heads_here), axis=1)
    by_head = cumul.transpose(0, 2, 1)
    lower = jnp.tril(jnp.ones((BLOCK, BLOCK), dtype=bool))
    spread = by_head[:, :, :, None] - by_head[:, :, None, :]
    weight = jnp.where(lower, jnp.exp(jnp.where(lower, spread, 0.0)), 0.0)
    scores = jnp.einsum("nthd,nshd->nhts", q_blocks, k_blocks, preferred_element_type=jnp.float32)
    probs = (scores * weight).astype(jnp.bfloat16)
    inner = jnp.einsum("nhts,nshe->nthe", probs, v_blocks, preferred_element_type=jnp.float32)
    k_weighted = (
        k_blocks.astype(jnp.float32) * jnp.exp(cumul[:, -1:, :] - cumul)[..., None]
    ).astype(jnp.bfloat16)
    contrib = jnp.einsum(
        "nshd,nshe->nhde", k_weighted, v_blocks, preferred_element_type=jnp.float32
    )
    totals = jnp.exp(cumul[:, -1, :])

    def advance(carry, items):
        state, prefix = carry
        factor, update = items
        return ((state * factor[:, None, None] + update, prefix * factor), (state, prefix))

    start_state = jnp.zeros((heads_here, head_size, head_size), jnp.float32)
    start_prefix = jnp.ones((heads_here,), jnp.float32)
    (dev_state, dev_total), (local_before, prefixes) = lax.scan(
        advance, (start_state, start_prefix), (totals, contrib)
    )
    _, incoming = prefix_2((dev_total, dev_state), "sp", join_states, (start_prefix, start_state))
    before = local_before + prefixes[:, :, None, None] * incoming[None]
    cross = jnp.einsum(
        "nthd,nhde->nthe", q_blocks.astype(jnp.float32), before, precision=lax.Precision.HIGHEST
    )
    cross = cross * jnp.exp(cumul)[..., None]
    result = (inner + cross).reshape(tok_rows, heads_here, head_size)
    result = row_norm(result, head_gain.reshape(heads_here, head_size)).reshape(
        tok_rows, heads_here * head_size
    )
    retained = (result * jax.nn.silu(gate_input.astype(jnp.float32))).astype(jnp.bfloat16)
    picked = retained
    mixed = lax.psum_scatter(
        jnp.dot(picked, out_weight, preferred_element_type=jnp.float32).astype(jnp.bfloat16),
        "tp",
        scatter_dimension=0,
        tiled=True,
    ).astype(jnp.float32)
    own_rows = lax.dynamic_slice_in_dim(residual, lax.axis_index("tp") * quarter, quarter, 0)
    rows_mid = (own_rows.astype(jnp.float32) + mixed).astype(jnp.bfloat16)
    own_normed = row_norm(rows_mid.astype(jnp.float32), mlp_gain).astype(jnp.bfloat16)
    normed = lax.all_gather(own_normed, "tp", axis=0, tiled=True)
    gate = jnp.dot(
        normed,
        lax.all_gather(gate_weight, "sp", axis=0, tiled=True),
        preferred_element_type=jnp.float32,
    )
    upvals = jnp.dot(
        normed,
        lax.all_gather(up_weight, "sp", axis=0, tiled=True),
        preferred_element_type=jnp.float32,
    )
    full_down = lax.all_gather(down_weight, "sp", axis=1, tiled=True)
    hidden = (jax.nn.silu(gate) * upvals).astype(jnp.bfloat16)
    picked = hidden
    ffn = lax.psum_scatter(
        jnp.dot(picked, full_down, preferred_element_type=jnp.float32).astype(jnp.bfloat16),
        "tp",
        scatter_dimension=0,
        tiled=True,
    ).astype(jnp.float32)
    return (rows_mid.astype(jnp.float32) + ffn).astype(jnp.bfloat16)


MESH = pl.DeviceIdType.MESH
XS = 2
CS = 2
F32 = jnp.float32
BF16 = jnp.bfloat16


def dot_nt(a, b):
    return lax.dot_general(a, b, (((1,), (1,)), ((), ())), preferred_element_type=F32)


def dot_nn(a, b):
    return lax.dot_general(a, b, (((1,), (0,)), ((), ())), preferred_element_type=F32)


def kernel(names, nz, nt, *refs):
    r = types.SimpleNamespace(**dict(zip(names, refs)))
    sp = lax.axis_index("sp")
    tp = lax.axis_index("tp")
    z, x = sp // XS, lax.rem(sp, XS)
    y, c = tp // CS, lax.rem(tp, CS)
    rows = r.q.shape[0]
    heads = r.ld.shape[0]
    hh = heads // XS
    hd = r.q.shape[1] // heads
    quarter = rows // nt
    share, width = r.wg.shape[2], r.wg.shape[3]
    group = XS * width
    ns = nz * XS
    zat = [z, z + 1 - 2 * lax.rem(z, 2), lax.rem(z + 2, nz), nz - 1 - z]

    def dev(zz, xx, yy, cc):
        return (zz * XS + xx, yy * CS + cc)

    x_peer = dev(z, 1 - x, y, c)
    c_peer = dev(z, x, y, 1 - c)

    barrier = pltpu.get_barrier_semaphore()
    peers = [dev(zat[e], x, y, k) for e in range(1, nz) for k in range(CS)]
    peers += [c_peer] + [dev(zat[e], 1 - x, y, c) for e in range(1, nz)]
    peers += [dev(z, 1 - x, y, k) for k in range(CS)]
    peers += [dev(z, x, 1 - y, k) for k in range(CS)]
    for peer in peers:
        pl.semaphore_signal(barrier, inc=1, device_id=peer, device_id_type=MESH)

    loads = {}

    def load(name, src, dst):
        loads[name] = pltpu.make_async_copy(src, dst, r.in_sem.at[len(loads)])
        loads[name].start()

    load("gw", r.gw_hbm, r.raw.at[0])
    load("uw", r.uw_hbm, r.raw.at[1])
    for name in ("ld", "q", "k", "v"):
        load(name, getattr(r, name + "_hbm"), getattr(r, name))
    load("dw", r.dw_hbm, r.slab.at[2])
    for name in ("g", "hg", "ow", "mg"):
        load(name, getattr(r, name + "_hbm"), getattr(r, name))
    mine = pl.multiple_of(tp * quarter, quarter)
    load("res", r.res_hbm.at[pl.ds(mine, quarter)], r.res)

    def remote(src, dst, send, recv, peer):
        return pltpu.make_async_remote_copy(
            src_ref=src,
            dst_ref=dst,
            send_sem=send,
            recv_sem=recv,
            device_id=peer,
            device_id_type=MESH,
        )

    def go(build):
        build().start()

    def sent(view, sem):
        remote(view, view, sem, sem, c_peer).wait_send()

    def piece(ref, m, zz):
        return ref.at[m, pl.ds(pl.multiple_of(zz * share, 16), share)]

    def slot(m, zz):
        return r.wg.at[m, zz * XS + x]

    own_copies = {}

    def take_own(m):
        own_copies[m] = pltpu.make_async_copy(piece(r.slab, m, z), slot(m, z), r.own_sem.at[m])
        own_copies[m].start()

    for m, name in enumerate(("gw", "uw")):
        loads[name].wait()
        for j in range(r.raw.shape[2] // 128):
            r.slab[m, j * 128 : (j + 1) * 128, :] = jnp.transpose(
                r.raw[m, :, j * 128 : (j + 1) * 128]
            )
        take_own(m)
    loads["dw"].wait()
    take_own(2)
    pl.semaphore_wait(barrier, len(peers))

    def hand(m):
        return lambda: remote(
            r.slab.at[m], r.partner.at[m], r.h_send, r.h_recv.at[m], c_peer
        )

    def weight(m, e, k):
        source = r.partner if k else r.slab
        return lambda: remote(
            piece(source, m, zat[e]),
            slot(m, z),
            r.w_send,
            r.w_recv.at[m, e - 1],
            dev(zat[e], x, y, k),
        )

    outer = jnp.logical_or(z == 0, z == nz - 1)
    outer_head = ((0, 1), (1, 1))
    outer_tail = ((2, 1), (0, 2), (0, 3), (1, 2), (1, 3))
    inner_head = ((0, 3), (0, 1), (1, 3), (1, 1))
    inner_tail = ((0, 2), (2, 1), (1, 2))

    def send_weights(plan, which=range(CS)):
        for m, e in plan:
            for k in which:
                weight(m, e, k)().start()

    def got_weight(m, e):
        weight(m, e, 0)().wait_recv()

    def forward(m, e):
        at = slot(m, zat[e])
        source = piece(r.slab, m, z) if e == 0 else at
        recv = r.f_recv.at[2 + e] if m == 2 else r.f_recv.at[m]
        return lambda: remote(source, at, r.f_send, recv, x_peer)

    def pass_on(m, e):
        if e:
            got_weight(m, e)
        go(forward(m, e))

    def pass_if(when, pieces):
        @pl.when(when)
        def _():
            for m, e in pieces:
                got_weight(m, e)
                forward(m, e)().start()

    near = ((0, 1), (1, 1))

    def got_forwards(m):
        view = r.wg.at[m, :nz]
        remote(view, view, r.f_send, r.f_recv.at[m], x_peer).wait_recv()

    @pl.when(c == 1)
    def _():
        for m in range(3):
            go(hand(m))

    @pl.when(jnp.logical_and(c == 0, outer))
    def _():
        send_weights(outer_head, (0,))

    @pl.when(jnp.logical_and(c == 0, jnp.logical_not(outer)))
    def _():
        send_weights(inner_head, (0,))

    for name in ("ld", "q", "k", "v"):
        loads[name].wait()
    ti = lax.broadcasted_iota(jnp.int32, (rows, rows), 0)
    si = lax.broadcasted_iota(jnp.int32, (rows, rows), 1)
    lower = si <= ti
    cumul = lax.dot_general(
        r.ld[...],
        (ti <= si).astype(F32),
        (((1,), (0,)), ((), ())),
        precision=lax.Precision.HIGHEST,
        preferred_element_type=F32,
    )
    half = hd // 2
    lane = lax.broadcasted_iota(jnp.int32, (1, hd), 1)
    low_half = lane < half
    index = jnp.where(low_half, lane, lane - half).astype(F32)
    freq = jnp.exp(index * (-math.log(10000.0) / (half - 1)))
    angles = (sp * rows + lax.broadcasted_iota(jnp.int32, (rows, hd), 0)).astype(F32) * freq
    cos = jnp.cos(angles)
    sin = jnp.sin(angles)
    sin = jnp.where(low_half, -sin, sin)
    for h in range(heads):
        cols = slice(h * hd, (h + 1) * hd)
        qf = r.q[:, cols].astype(F32)
        kf = r.k[:, cols].astype(F32)
        vb = r.v[:, cols]
        qb = (qf * cos + pltpu.roll(qf, half, 1) * sin).astype(BF16)
        kb = ((kf * cos + pltpu.roll(kf, half, 1) * sin) * hd ** (-0.5)).astype(BF16)
        along = jnp.broadcast_to(cumul[h : h + 1, :], (rows, rows))
        cum = jnp.transpose(along)
        spread = cum - along
        weight_ts = jnp.where(lower, jnp.exp(jnp.where(lower, spread, 0.0)), 0.0)
        probs = (dot_nt(qb, kb) * weight_ts).astype(BF16)
        r.inner[:, cols] = dot_nn(probs, vb)
        last = cum[rows - 1 :, :]
        kw = kb.astype(F32) * jnp.exp(last - cum)
        r.c_out[h] = dot_nn(jnp.transpose(kw).astype(BF16), vb).astype(BF16)
        r.t_out[h] = jnp.broadcast_to(jnp.exp(last), r.t_out.shape[1:])
        r.qrot[:, cols] = qb
        r.cumx[:, cols] = jnp.exp(cum)

    my_h, its_h = pl.ds(x * hh, hh), pl.ds((1 - x) * hh, hh)
    x_one, c_one = dev(z, 1 - x, y, 1), dev(z, x, y, 1)

    def cross_c(k):
        return lambda: remote(
            r.c_out.at[its_h], r.ci.at[1, k], r.cx_send.at[0], r.cx_recv.at[0, k], x_one
        )

    def cross_t(k):
        return lambda: remote(
            r.t_out.at[its_h], r.ti.at[1, k], r.cx_send.at[1], r.cx_recv.at[1, k], x_one
        )

    go(cross_c(c))
    go(cross_t(c))

    def near_c():
        return remote(r.c_out.at[my_h], r.ci.at[0, 0], r.cc_send.at[0], r.cc_recv.at[0], c_one)

    def near_t():
        return remote(r.t_out.at[my_h], r.ti.at[0, 0], r.cc_send.at[1], r.cc_recv.at[1], c_one)

    def chain():
        up = jnp.minimum(z + 1, nz - 1)
        return remote(r.ch_out, r.ch_in, r.ch_send, r.ch_recv, dev(up, x, y, 1))

    def state_x(k):
        return lambda: remote(
            r.so.at[1, k], r.s_in.at[1], r.so_send.at[k], r.s_recv.at[1], dev(z, 1 - x, y, k)
        )

    def state_c():
        return remote(
            r.so.at[0, 0], r.s_in.at[0], r.so_send.at[2], r.s_recv.at[0], dev(z, x, y, 0)
        )

    @pl.when(c == 0)
    def _():
        go(near_c)
        go(near_t)
        for m in range(3):
            hand(m)().wait_recv()

        @pl.when(outer)
        def _():
            send_weights(outer_head, (1,))
            send_weights(outer_tail)

        @pl.when(jnp.logical_not(outer))
        def _():
            send_weights(inner_head, (1,))
            send_weights(inner_tail)

    late = z >= nz // 2
    first = x == 0

    def pass_own(when):
        @pl.when(when)
        def _():
            for m in range(2):
                forward(m, 0)().start()

    pass_own(late)

    @pl.when(c == 1)
    def _():
        r.ci[0, 1] = r.c_out[my_h]
        r.ti[0, 1] = r.t_out[my_h]
        near_c().wait_recv()
        near_t().wait_recv()
        for k in range(CS):
            cross_c(k)().wait_recv()
            cross_t(k)().wait_recv()
        for k in range(CS):
            for i in range(hh):
                own_c, own_t = r.ci[0, k, i].astype(F32), r.ti[0, k, i][:1]
                other_c, other_t = r.ci[1, k, i].astype(F32), r.ti[1, k, i][:1]
                early_c = jnp.where(first, own_c, other_c)
                late_c = jnp.where(first, other_c, own_c)
                late_t = jnp.where(first, other_t, own_t)
                r.plane[k, i] = late_t * early_c + late_c

        pass_if(late, near)

        @pl.when(z == 0)
        def _():
            r.ch_in[...] = jnp.zeros(r.ch_in.shape, BF16)

        @pl.when(z > 0)
        def _():
            chain().wait_recv()

        for k in range(CS):
            for i in range(hh):
                both_t = r.ti[0, k, i][:1] * r.ti[1, k, i][:1]
                state = r.ch_in[k, i].astype(F32)
                r.ch_out[k, i] = (both_t * state + r.plane[k, i]).astype(BF16)

        @pl.when(z < nz - 1)
        def _():
            go(chain)

        for k in range(CS):
            for i in range(hh):
                early_c = jnp.where(first, r.ci[0, k, i], r.ci[1, k, i]).astype(F32)
                early_t = jnp.where(first, r.ti[0, k, i][:1], r.ti[1, k, i][:1])
                state = r.ch_in[k, i].astype(F32)
                after = early_t * state + early_c
                r.so[0, k, i] = jnp.where(first, state, after).astype(BF16)
                r.so[1, k, i] = jnp.where(first, after, state).astype(BF16)
        for k in range(CS):
            go(state_x(k))
        go(state_c)
        r.s_in[0] = r.so[0, 1]

    @pl.when(c == 0)
    def _():
        pass_if(late, near)
        state_c().wait_recv()

    pass_own(jnp.logical_not(late))
    state_x(0)().wait_recv()
    loads["g"].wait()
    loads["hg"].wait()
    for h in range(heads):
        cols = slice(h * hd, (h + 1) * hd)
        state = r.s_in[lax.rem(x + h // hh, XS), h % hh]
        ret = r.inner[:, cols] + r.cumx[:, cols] * dot_nn(r.qrot[:, cols], state)
        scale = lax.rsqrt(jnp.mean(ret * ret, axis=-1, keepdims=True) + EPS)
        gf = r.g[:, cols].astype(F32)
        r.retained[:, cols] = (
            ret * scale * r.hg[:, cols] * (gf / (1.0 + jnp.exp(-gf)))
        ).astype(BF16)
    loads["ow"].wait()

    def mix_c():
        return remote(r.mc_out, r.mc_in, r.mix_send.at[0], r.mix_recv.at[0], c_peer)

    def mix_y():
        return remote(
            r.my_out, r.my_in, r.mix_send.at[1], r.mix_recv.at[1], dev(z, x, 1 - y, c)
        )

    def mix_part(cc):
        picked = [
            r.retained[pl.ds(pl.multiple_of((yy * CS + cc) * quarter, quarter), quarter), :]
            for yy in range(nt // CS)
        ]
        part = dot_nn(jnp.concatenate(picked, axis=0), r.ow[...])
        return part.reshape(nt // CS, quarter, part.shape[1])

    r.mc_out[...] = mix_part(1 - c).astype(BF16)
    go(mix_c)
    r.mix_own[...] = mix_part(c)
    mix_c().wait_recv()
    r.my_out[...] = (r.mix_own[1 - y] + r.mc_in[1 - y].astype(F32)).astype(BF16)
    go(mix_y)
    early = jnp.logical_not(late)
    pass_if(early, near)
    pass_on(0, 2)
    pass_if(late, ((0, 3),))
    mixed = r.mix_own[y] + r.mc_in[y].astype(F32)
    mix_y().wait_recv()
    mixed += r.my_in[...].astype(F32)
    loads["res"].wait()
    loads["mg"].wait()
    mid = (r.res[...].astype(F32) + mixed).astype(BF16).astype(F32)
    for g in range(nz):
        for u in range(XS):
            at = g * group + u * width
            r.acc[g, u] = mid[:, at : at + width]
    r.normed[z, tp] = (
        mid * lax.rsqrt(jnp.mean(mid * mid, axis=-1, keepdims=True) + EPS) * r.mg[...]
    ).astype(BF16)

    def rows_c():
        rows_at = r.normed.at[z, tp]
        return remote(rows_at, rows_at, r.nc_send, r.nc_recv, c_peer)

    def rows_of(zz, yy, j):
        return r.normed.at[zz, yy * CS + j]

    def rows_z(k, j):
        to = zat[2] if k == 0 else zat[1]
        zz = zat[2] if k == 2 else z
        return lambda: remote(
            rows_of(zz, y, j),
            rows_of(zz, y, j),
            r.nz_send,
            r.nz_recv.at[k, j],
            dev(to, x, y, 1),
        )

    def rows_y(e, j):
        return lambda: remote(
            rows_of(zat[e], y, j),
            rows_of(zat[e], y, j),
            r.ny_send,
            r.ny_recv.at[e, j],
            dev(z, x, 1 - y, 1),
        )

    def rows_d(e, v, j):
        def build():
            rows_at = rows_of(zat[e], 1 - y if v else y, j)
            return remote(
                rows_at, rows_at, r.nd_send.at[v], r.nd_recv.at[v, e], dev(z, x, y, 0)
            )

        return build

    def got_rows(e, v):
        view = r.normed.at[zat[e], pl.ds((1 - y if v else y) * CS, CS)]
        remote(view, view, r.nd_send.at[v], r.nd_recv.at[v, e], c_peer).wait_recv()

    go(rows_c)

    def send_down(if_outer, if_inner):
        @pl.when(outer)
        def _():
            send_weights(((2, if_outer),))

        @pl.when(jnp.logical_not(outer))
        def _():
            send_weights(((2, if_inner),))

    @pl.when(c == 1)
    def _():
        for j in (1, 0):
            if j == 0:
                rows_c().wait_recv()
            for k in range(2):
                go(rows_z(k, j))
            go(rows_y(0, j))

    @pl.when(c == 0)
    def _():
        rows_c().wait_recv()

    pass_if(early, ((0, 3),))
    own_copies[2].wait()
    pass_on(2, 0)
    pass_on(1, 3)

    @pl.when(c == 1)
    def _():
        for j in (1, 0):
            rows_z(1, j)().wait_recv()
            go(rows_y(1, j))
            go(rows_d(1, 0, j))
        for j in (1, 0):
            rows_y(0, j)().wait_recv()
            go(rows_d(0, 1, j))
        for j in (1, 0):
            rows_z(0, j)().wait_recv()
            go(rows_z(2, j))
            go(rows_y(2, j))
            go(rows_d(2, 0, j))

    pass_on(1, 2)
    pass_on(2, 1)

    @pl.when(c == 0)
    def _():
        got_rows(2, 0)
        send_down(2, 3)

    @pl.when(c == 1)
    def _():
        for j in (1, 0):
            rows_y(1, j)().wait_recv()
            go(rows_d(1, 1, j))
        for j in (1, 0):
            rows_z(2, j)().wait_recv()
            go(rows_y(3, j))
            go(rows_d(3, 0, j))

    @pl.when(c == 0)
    def _():
        got_rows(3, 0)
        send_down(3, 2)
        for e, v in ((1, 0), (0, 1), (1, 1)):
            got_rows(e, v)

    def project(m, half_z):
        block = r.normed[pl.ds(2 * half_z, 2)].reshape(2 * rows, r.normed.shape[3])
        total = dot_nt(block[:, :width], r.wg[m, 0])
        for s in range(1, ns):
            total += dot_nt(block[:, s * width : (s + 1) * width], r.wg[m, s])
        return total

    def gate_rows(half_z):
        gate = project(0, half_z)
        r.gated[half_z] = gate / (1.0 + jnp.exp(-gate))

    def half_at(half_z):
        return pl.ds(pl.multiple_of(half_z * 2 * rows, 2 * rows), 2 * rows)

    def hand_hidden(i):
        at = half_at(own_half if i == 0 else 1 - own_half)
        return lambda: remote(
            r.hidden.at[0, at], r.hidden.at[1, at], r.hx_send, r.hx_recv.at[i], x_peer
        )

    def up_rows(i):
        half_z = own_half if i == 0 else 1 - own_half
        r.hidden[0, half_at(half_z), :] = (r.gated[half_z] * project(1, half_z)).astype(BF16)
        go(hand_hidden(i))

    own_half = z // 2
    own_copies[0].wait()
    got_forwards(0)
    gate_rows(own_half)

    @pl.when(c == 1)
    def _():
        for e in (2, 3):
            for j in (1, 0):
                rows_y(e, j)().wait_recv()
                go(rows_d(e, 1, j))

    own_copies[1].wait()
    got_forwards(1)
    up_rows(0)

    @pl.when(c == 0)
    def _():
        for e in (2, 3):
            got_rows(e, 1)

    gate_rows(1 - own_half)
    up_rows(1)

    low = c == 0

    def t1(b, u):
        return lambda: remote(
            r.s1.at[b, u], r.r1.at[b, u], r.t1_send, r.t1_recv.at[b, u], c_peer
        )

    def t2(b, u):
        return lambda: remote(
            r.s2.at[b, u],
            r.r2.at[b, u],
            r.t2_send,
            r.t2_recv.at[b, u],
            dev(z, x, 1 - y, c),
        )

    def unit(b, u):
        return XS * b + u if b < 2 else b + 2

    def t3(b, u, e):
        if b > 1 and u:
            return lambda: remote(
                r.s3x.at[b - 2, e],
                r.r3x.at[b - 2, e],
                r.t3x_send,
                r.t3x_recv.at[b - 2],
                dev(zat[e], 1 - x, y, c),
            )
        return lambda: remote(
            r.s3.at[unit(b, u), e - 1],
            r.r3.at[unit(b, u), e - 1],
            r.t3_send,
            r.t3_recv.at[unit(b, u)],
            dev(zat[e], x, y, c),
        )

    def side(u):
        return 1 - x if u else x

    def compute(b, u):
        if b < 2:
            if u:
                forward(2, b)().wait_recv()
            part = dot_nn(r.hidden[0], r.wg[2, zat[b] * XS + side(u)])
        else:
            part = dot_nn(r.hidden[u], r.wg[2, zat[b] * XS + x])
        for zz in range(nz):
            for yy in range(nt // CS):
                at = zz * rows + yy * CS * quarter
                even = part[at : at + quarter]
                odd = part[at + quarter : at + 2 * quarter]
                r.keep[b, u, yy, zz] = jnp.where(low, even, odd)
                r.s1[b, u, yy, zz] = jnp.where(low, odd, even).astype(BF16)
        go(t1(b, u))

    def second(b, u):
        t1(b, u)().wait_recv()
        r.s2[b, u] = (r.keep[b, u, 1 - y] + r.r1[b, u, 1 - y].astype(F32)).astype(BF16)
        go(t2(b, u))
        r.keep[b, u, y] = r.keep[b, u, y] + r.r1[b, u, y].astype(F32)

    def third(b, u):
        t2(b, u)().wait_recv()
        def value(e):
            return r.keep[b, u, y, zat[e]] + r.r2[b, u, zat[e]].astype(F32)

        if b > 1 and u:
            for e in (3, 2, 1, 0):
                r.s3x[b - 2, e] = value(e).astype(BF16)
                go(t3(b, u, e))
            return
        for e in (3, 2, 1):
            r.s3[unit(b, u), e - 1] = value(e).astype(BF16)
            go(t3(b, u, e))
        r.acc[zat[b], side(u)] = r.acc[zat[b], side(u)] + value(0)

    def last(b, u):
        if b > 1 and u:
            view = r.r3x.at[b - 2]
            remote(view, view, r.t3x_send, r.t3x_recv.at[b - 2], c_peer).wait_recv()
            for e in range(nz):
                g = zat[b ^ e]
                r.acc[g, 1 - x] = r.acc[g, 1 - x] + r.r3x[b - 2, e].astype(F32)
            return
        view = r.r3.at[unit(b, u)]
        remote(view, view, r.t3_send, r.t3_recv.at[unit(b, u)], c_peer).wait_recv()
        for e in (1, 3, 2):
            g = zat[b ^ e]
            r.acc[g, side(u)] = r.acc[g, side(u)] + r.r3[unit(b, u), e - 1].astype(F32)

    def other_hidden():
        for i in range(2):
            hand_hidden(i)().wait_recv()

    for b in range(2):
        for u in range(XS):
            compute(b, u)
    for b in range(2):
        for u in range(XS):
            second(b, u)
    got_weight(2, 3)
    compute(3, 0)
    third(0, 0)
    third(0, 1)
    second(3, 0)
    third(1, 0)
    got_weight(2, 2)
    compute(2, 0)
    other_hidden()
    compute(3, 1)
    compute(2, 1)
    third(1, 1)
    second(2, 0)
    second(3, 1)
    second(2, 1)
    third(3, 0)
    third(2, 0)
    third(3, 1)
    third(2, 1)
    for b in (0, 1):
        for u in range(XS):
            last(b, u)
    for b, u in ((3, 0), (2, 0), (3, 1), (2, 1)):
        last(b, u)
    for g in range(nz):
        for u in range(XS):
            at = g * group + u * width
            r.out[:, at : at + width] = r.acc[g, u].astype(BF16)

    sent(r.wg.at[:2, : nz + 1], r.f_send)
    sent(r.hidden.at[0], r.hx_send)
    sent(r.s1, r.t1_send)
    sent(r.s2, r.t2_send)
    sent(r.s3, r.t3_send)
    sent(r.s3x, r.t3x_send)
    for build in (cross_c(c), cross_t(c), rows_c, mix_c, mix_y):
        build().wait_send()

    @pl.when(c == 0)
    def _():
        sent(r.wg.at[:, : CS * (nz - 1)], r.w_send)
        near_c().wait_send()
        near_t().wait_send()

    @pl.when(c == 1)
    def _():
        sent(r.slab, r.h_send)
        sent(r.normed.at[:3, :CS], r.nz_send)
        sent(r.normed.at[:CS], r.ny_send)
        sent(r.normed.at[: nz - 1, :CS], r.nd_send.at[0])
        sent(r.normed.at[:CS], r.nd_send.at[1])
        for build in (state_x(0), state_x(1), state_c):
            build().wait_send()

    @pl.when(jnp.logical_and(c == 1, z < nz - 1))
    def _():
        chain().wait_send()


def fast_body(
    queries,
    key_rows,
    value_rows,
    gate_input,
    log_decay,
    head_gain,
    out_weight,
    residual,
    mlp_gain,
    gate_weight,
    up_weight,
    down_weight,
):
    rows, wide = queries.shape
    heads = log_decay.shape[1]
    hd = wide // heads
    model = residual.shape[1]
    ns, nt = lax.axis_size("sp"), lax.axis_size("tp")
    nz = ns // XS
    quarter = rows // nt
    width, units = gate_weight.shape
    share = units // nz
    hh = heads // XS
    vmem = pltpu.VMEM
    dma = pltpu.SemaphoreType.DMA
    operands = {
        "q_hbm": queries,
        "k_hbm": key_rows,
        "v_hbm": value_rows,
        "g_hbm": gate_input,
        "ld_hbm": log_decay.T,
        "hg_hbm": head_gain.reshape(1, wide),
        "res_hbm": residual,
        "mg_hbm": mlp_gain.reshape(1, model),
        "ow_hbm": out_weight,
        "gw_hbm": gate_weight,
        "uw_hbm": up_weight,
        "dw_hbm": down_weight,
    }
    scratch = {
        "q": vmem((rows, wide), BF16),
        "k": vmem((rows, wide), BF16),
        "v": vmem((rows, wide), BF16),
        "g": vmem((rows, wide), BF16),
        "ld": vmem((heads, rows), F32),
        "hg": vmem((1, wide), F32),
        "res": vmem((quarter, model), BF16),
        "mg": vmem((1, model), F32),
        "ow": vmem(out_weight.shape, BF16),
        "raw": vmem((2, width, units), BF16),
        "slab": vmem((3, units, width), BF16),
        "partner": vmem((3, units, width), BF16),
        "wg": vmem((3, ns, share, width), BF16),
        "qrot": vmem((rows, wide), BF16),
        "inner": vmem((rows, wide), F32),
        "cumx": vmem((rows, wide), F32),
        "c_out": vmem((heads, hd, hd), BF16),
        "t_out": vmem((heads, 8, hd), F32),
        "ci": vmem((XS, CS, hh, hd, hd), BF16),
        "ti": vmem((XS, CS, hh, 8, hd), F32),
        "plane": vmem((CS, hh, hd, hd), F32),
        "ch_in": vmem((CS, hh, hd, hd), BF16),
        "ch_out": vmem((CS, hh, hd, hd), BF16),
        "so": vmem((XS, CS, hh, hd, hd), BF16),
        "s_in": vmem((XS, hh, hd, hd), BF16),
        "retained": vmem((rows, wide), BF16),
        "mc_out": vmem((nt // CS, quarter, model), BF16),
        "mc_in": vmem((nt // CS, quarter, model), BF16),
        "mix_own": vmem((nt // CS, quarter, model), F32),
        "my_out": vmem((quarter, model), BF16),
        "my_in": vmem((quarter, model), BF16),
        "acc": vmem((nz, XS, quarter, width), F32),
        "normed": vmem((nz, nt, quarter, model), BF16),
        "gated": vmem((nz // 2, 2 * rows, share), F32),
        "hidden": vmem((XS, nz * rows, share), BF16),
        "keep": vmem((nz, XS, nt // CS, nz, quarter, width), F32),
        "s1": vmem((nz, XS, nt // CS, nz, quarter, width), BF16),
        "r1": vmem((nz, XS, nt // CS, nz, quarter, width), BF16),
        "s2": vmem((nz, XS, nz, quarter, width), BF16),
        "r2": vmem((nz, XS, nz, quarter, width), BF16),
        "s3": vmem((nz + 2, nz - 1, quarter, width), BF16),
        "r3": vmem((nz + 2, nz - 1, quarter, width), BF16),
        "s3x": vmem((2, nz, quarter, width), BF16),
        "r3x": vmem((2, nz, quarter, width), BF16),
        "in_sem": dma((len(operands),)),
        "own_sem": dma((3,)),
        "h_send": dma,
        "h_recv": dma((3,)),
        "w_send": dma,
        "w_recv": dma((3, nz - 1)),
        "f_send": dma,
        "f_recv": dma((4,)),
        "cx_send": dma((2,)),
        "cx_recv": dma((2, CS)),
        "cc_send": dma((2,)),
        "cc_recv": dma((2,)),
        "ch_send": dma,
        "ch_recv": dma,
        "so_send": dma((3,)),
        "s_recv": dma((XS,)),
        "mix_send": dma((2,)),
        "mix_recv": dma((2,)),
        "nc_send": dma,
        "nc_recv": dma,
        "nz_send": dma,
        "nz_recv": dma((3, CS)),
        "ny_send": dma,
        "ny_recv": dma((nz, CS)),
        "nd_send": dma((2,)),
        "nd_recv": dma((2, nz)),
        "t1_send": dma,
        "t1_recv": dma((nz, XS)),
        "t2_send": dma,
        "t2_recv": dma((nz, XS)),
        "t3_send": dma,
        "t3_recv": dma((nz + 2,)),
        "t3x_send": dma,
        "t3x_recv": dma((2,)),
        "hx_send": dma,
        "hx_recv": dma((2,)),
    }
    names = list(operands) + ["out"] + list(scratch)
    return pl.pallas_call(
        functools.partial(kernel, names, nz, nt),
        out_shape=pltpu.VMEM((quarter, model), BF16),
        in_specs=[pl.BlockSpec(memory_space=pl.ANY)] * len(operands),
        out_specs=pl.BlockSpec(memory_space=pltpu.VMEM),
        scratch_shapes=list(scratch.values()),
        compiler_params=pltpu.CompilerParams(
            collective_id=0, has_side_effects=True, vmem_limit_bytes=60 * 1024 * 1024
        ),
    )(*operands.values())


def fits(mesh, queries, log_decay, gate_weight):
    ns, nt = mesh.shape["sp"], mesh.shape["tp"]
    tokens, wide = queries.shape
    if ns % XS or ns // XS != 4 or nt != 2 * CS or tokens // ns != BLOCK:
        return False
    nz = ns // XS
    hidden = gate_weight.shape[1] // nt
    return (
        gate_weight.shape[0] // ns % 128 == 0
        and hidden % (16 * nz) == 0
        and wide // log_decay.shape[1] == 128
        and BLOCK % (16 * nt) == 0
        and hidden % 128 == 0
        and log_decay.shape[1] // nt % XS == 0
    )


def solution(mesh):
    def run(*args):
        good = fits(mesh, args[0], args[4], args[9])
        return jax.shard_map(
            fast_body if good else body,
            mesh=mesh,
            in_specs=(
                P("sp", "tp"),
                P("sp", "tp"),
                P("sp", "tp"),
                P("sp", "tp"),
                P("sp", "tp"),
                P("tp"),
                P("tp", None),
                P("sp", None),
                P(),
                P("sp", "tp"),
                P("sp", "tp"),
                P("tp", "sp"),
            ),
            out_specs=P(("sp", "tp"), None),
            check_vma=False,
        )(*args)

    return run
```

```python
import functools
import math
import types

import jax
import jax.numpy as jnp
from jax import lax
from jax.experimental import pallas as pl
from jax.experimental.pallas import tpu as pltpu
from jax.sharding import PartitionSpec as P

BLOCK = 128


EPS = 1e-06


def prefix_2(x, axis, join, neutral):
    place = lax.axis_index(axis)
    gathered = jax.tree.map(
        lambda a, kind: lax.all_gather(a.astype(kind), axis), x, (jnp.bfloat16, jnp.bfloat16)
    )
    state = jax.tree.map(lambda a, e: jnp.zeros_like(a) + jnp.asarray(e, a.dtype), x, neutral)

    def one(step, state):
        return join(
            state,
            jax.tree.map(
                lambda a, own: lax.dynamic_index_in_dim(a, step, 0, False).astype(own.dtype),
                gathered,
                x,
            ),
        )

    return lax.fori_loop(0, place, one, state)


def rotate(values_in, positions):
    half = values_in.shape[-1] // 2
    freq = 10000.0 ** (-jnp.linspace(0.0, 1.0, half, dtype=jnp.float32))
    angles = positions * freq
    angles = jnp.concatenate([angles, angles], axis=-1)
    first = values_in[..., :half]
    second = values_in[..., half:]
    turned = jnp.concatenate([-second, first], axis=-1)
    return values_in * jnp.cos(angles) + turned * jnp.sin(angles)


def row_norm(stream, gain):
    return stream * lax.rsqrt(jnp.mean(stream * stream, axis=-1, keepdims=True) + EPS) * gain


def join_states(earlier, later):
    return (earlier[0] * later[0], later[0][:, None, None] * earlier[1] + later[1])


def body(
    queries,
    key_rows,
    value_rows,
    gate_input,
    log_decay,
    head_gain,
    out_weight,
    residual,
    mlp_gain,
    gate_weight,
    up_weight,
    down_weight,
):
    tok_rows = queries.shape[0]
    heads_here = log_decay.shape[1]
    head_size = head_gain.shape[0] // heads_here
    quarter = tok_rows // lax.axis_size("tp")
    offset = lax.axis_index("sp") * tok_rows
    positions = (offset + lax.iota(jnp.int32, tok_rows)).astype(jnp.float32)[:, None, None]
    q_rot = rotate(
        queries.reshape(tok_rows, heads_here, head_size).astype(jnp.float32), positions
    ).astype(jnp.bfloat16)
    k_rot = (
        rotate(key_rows.reshape(tok_rows, heads_here, head_size).astype(jnp.float32), positions)
        * head_size ** (-0.5)
    ).astype(jnp.bfloat16)
    blocks = tok_rows // BLOCK
    q_blocks = q_rot.reshape(blocks, BLOCK, heads_here, head_size)
    k_blocks = k_rot.reshape(blocks, BLOCK, heads_here, head_size)
    v_blocks = value_rows.reshape(blocks, BLOCK, heads_here, head_size)
    cumul = jnp.cumsum(log_decay.reshape(blocks, BLOCK, heads_here), axis=1)
    by_head = cumul.transpose(0, 2, 1)
    lower = jnp.tril(jnp.ones((BLOCK, BLOCK), dtype=bool))
    spread = by_head[:, :, :, None] - by_head[:, :, None, :]
    weight = jnp.where(lower, jnp.exp(jnp.where(lower, spread, 0.0)), 0.0)
    scores = jnp.einsum("nthd,nshd->nhts", q_blocks, k_blocks, preferred_element_type=jnp.float32)
    probs = (scores * weight).astype(jnp.bfloat16)
    inner = jnp.einsum("nhts,nshe->nthe", probs, v_blocks, preferred_element_type=jnp.float32)
    k_weighted = (
        k_blocks.astype(jnp.float32) * jnp.exp(cumul[:, -1:, :] - cumul)[..., None]
    ).astype(jnp.bfloat16)
    contrib = jnp.einsum(
        "nshd,nshe->nhde", k_weighted, v_blocks, preferred_element_type=jnp.float32
    )
    totals = jnp.exp(cumul[:, -1, :])

    def advance(carry, items):
        state, prefix = carry
        factor, update = items
        return ((state * factor[:, None, None] + update, prefix * factor), (state, prefix))

    start_state = jnp.zeros((heads_here, head_size, head_size), jnp.float32)
    start_prefix = jnp.ones((heads_here,), jnp.float32)
    (dev_state, dev_total), (local_before, prefixes) = lax.scan(
        advance, (start_state, start_prefix), (totals, contrib)
    )
    _, incoming = prefix_2((dev_total, dev_state), "sp", join_states, (start_prefix, start_state))
    before = local_before + prefixes[:, :, None, None] * incoming[None]
    cross = jnp.einsum(
        "nthd,nhde->nthe", q_blocks.astype(jnp.float32), before, precision=lax.Precision.HIGHEST
    )
    cross = cross * jnp.exp(cumul)[..., None]
    result = (inner + cross).reshape(tok_rows, heads_here, head_size)
    result = row_norm(result, head_gain.reshape(heads_here, head_size)).reshape(
        tok_rows, heads_here * head_size
    )
    retained = (result * jax.nn.silu(gate_input.astype(jnp.float32))).astype(jnp.bfloat16)
    picked = retained
    mixed = lax.psum_scatter(
        jnp.dot(picked, out_weight, preferred_element_type=jnp.float32).astype(jnp.bfloat16),
        "tp",
        scatter_dimension=0,
        tiled=True,
    ).astype(jnp.float32)
    own_rows = lax.dynamic_slice_in_dim(residual, lax.axis_index("tp") * quarter, quarter, 0)
    rows_mid = (own_rows.astype(jnp.float32) + mixed).astype(jnp.bfloat16)
    own_normed = row_norm(rows_mid.astype(jnp.float32), mlp_gain).astype(jnp.bfloat16)
    normed = lax.all_gather(own_normed, "tp", axis=0, tiled=True)
    gate = jnp.dot(
        normed,
        lax.all_gather(gate_weight, "sp", axis=0, tiled=True),
        preferred_element_type=jnp.float32,
    )
    upvals = jnp.dot(
        normed,
        lax.all_gather(up_weight, "sp", axis=0, tiled=True),
        preferred_element_type=jnp.float32,
    )
    full_down = lax.all_gather(down_weight, "sp", axis=1, tiled=True)
    hidden = (jax.nn.silu(gate) * upvals).astype(jnp.bfloat16)
    picked = hidden
    ffn = lax.psum_scatter(
        jnp.dot(picked, full_down, preferred_element_type=jnp.float32).astype(jnp.bfloat16),
        "tp",
        scatter_dimension=0,
        tiled=True,
    ).astype(jnp.float32)
    return (rows_mid.astype(jnp.float32) + ffn).astype(jnp.bfloat16)


MESH = pl.DeviceIdType.MESH
XS = 2
CS = 2
F32 = jnp.float32
BF16 = jnp.bfloat16


def dot_nt(a, b):
    return lax.dot_general(a, b, (((1,), (1,)), ((), ())), preferred_element_type=F32)


def dot_nn(a, b):
    return lax.dot_general(a, b, (((1,), (0,)), ((), ())), preferred_element_type=F32)


def kernel(names, nz, nt, *refs):
    r = types.SimpleNamespace(**dict(zip(names, refs)))
    sp = lax.axis_index("sp")
    tp = lax.axis_index("tp")
    z, x = sp // XS, lax.rem(sp, XS)
    y, c = tp // CS, lax.rem(tp, CS)
    rows = r.q.shape[0]
    heads = r.ld.shape[0]
    hh = heads // XS
    hd = r.q.shape[1] // heads
    quarter = rows // nt
    share, width = r.wg.shape[2], r.wg.shape[3]
    group = XS * width
    ns = nz * XS
    zat = [z, z + 1 - 2 * lax.rem(z, 2), lax.rem(z + 2, nz), nz - 1 - z]

    def dev(zz, xx, yy, cc):
        return (zz * XS + xx, yy * CS + cc)

    x_peer = dev(z, 1 - x, y, c)
    c_peer = dev(z, x, y, 1 - c)

    barrier = pltpu.get_barrier_semaphore()
    peers = [dev(zat[e], x, y, k) for e in range(1, nz) for k in range(CS)]
    peers += [c_peer] + [dev(zat[e], 1 - x, y, c) for e in range(1, nz)]
    peers += [dev(z, 1 - x, y, k) for k in range(CS)]
    peers += [dev(z, x, 1 - y, k) for k in range(CS)]
    for peer in peers:
        pl.semaphore_signal(barrier, inc=1, device_id=peer, device_id_type=MESH)

    loads = {}

    def load(name, src, dst):
        loads[name] = pltpu.make_async_copy(src, dst, r.in_sem.at[len(loads)])
        loads[name].start()

    load("gw", r.gw_hbm, r.raw.at[0])
    load("uw", r.uw_hbm, r.raw.at[1])
    for name in ("ld", "q", "k", "v"):
        load(name, getattr(r, name + "_hbm"), getattr(r, name))
    load("dw", r.dw_hbm, r.slab.at[2])
    for name in ("g", "hg", "ow", "mg"):
        load(name, getattr(r, name + "_hbm"), getattr(r, name))
    mine = pl.multiple_of(tp * quarter, quarter)
    load("res", r.res_hbm.at[pl.ds(mine, quarter)], r.res)

    def remote(src, dst, send, recv, peer):
        return pltpu.make_async_remote_copy(
            src_ref=src,
            dst_ref=dst,
            send_sem=send,
            recv_sem=recv,
            device_id=peer,
            device_id_type=MESH,
        )

    def go(build):
        build().start()

    def sent(view, sem):
        remote(view, view, sem, sem, c_peer).wait_send()

    def piece(ref, m, zz):
        return ref.at[m, pl.ds(pl.multiple_of(zz * share, 16), share)]

    def slot(m, zz):
        return r.wg.at[m, zz * XS + x]

    own_copies = {}

    def take_own(m):
        own_copies[m] = pltpu.make_async_copy(piece(r.slab, m, z), slot(m, z), r.own_sem.at[m])
        own_copies[m].start()

    for m, name in enumerate(("gw", "uw")):
        loads[name].wait()
        for j in range(r.raw.shape[2] // 128):
            r.slab[m, j * 128 : (j + 1) * 128, :] = jnp.transpose(
                r.raw[m, :, j * 128 : (j + 1) * 128]
            )
        take_own(m)
    loads["dw"].wait()
    take_own(2)
    pl.semaphore_wait(barrier, len(peers))

    def hand(m):
        return lambda: remote(
            r.slab.at[m], r.partner.at[m], r.h_send, r.h_recv.at[m], c_peer
        )

    def weight(m, e, k):
        source = r.partner if k else r.slab
        return lambda: remote(
            piece(source, m, zat[e]),
            slot(m, z),
            r.w_send,
            r.w_recv.at[m, e - 1],
            dev(zat[e], x, y, k),
        )

    outer = jnp.logical_or(z == 0, z == nz - 1)
    outer_head = ((0, 1), (1, 1))
    outer_tail = ((2, 1), (0, 2), (0, 3), (1, 2), (1, 3))
    inner_head = ((0, 3), (0, 1), (1, 3), (1, 1))
    inner_tail = ((2,1),(0,2),(1,2))

    def send_weights(plan, which=range(CS)):
        for m, e in plan:
            for k in which:
                weight(m, e, k)().start()

    def got_weight(m, e):
        weight(m, e, 0)().wait_recv()

    def forward(m, e):
        at = slot(m, zat[e])
        source = piece(r.slab, m, z) if e == 0 else at
        recv = r.f_recv.at[2 + e] if m == 2 else r.f_recv.at[m]
        return lambda: remote(source, at, r.f_send, recv, x_peer)

    def pass_on(m, e):
        if e:
            got_weight(m, e)
        go(forward(m, e))

    def pass_if(when, pieces):
        @pl.when(when)
        def _():
            for m, e in pieces:
                got_weight(m, e)
                forward(m, e)().start()

    near = ((0, 1), (1, 1))

    def got_forwards(m):
        view = r.wg.at[m, :nz]
        remote(view, view, r.f_send, r.f_recv.at[m], x_peer).wait_recv()

    @pl.when(c == 1)
    def _():
        for m in range(3):
            go(hand(m))

    @pl.when(jnp.logical_and(c == 0, outer))
    def _():
        send_weights(outer_head, (0,))

    @pl.when(jnp.logical_and(c == 0, jnp.logical_not(outer)))
    def _():
        send_weights(inner_head, (0,))

    for name in ("ld", "q", "k", "v"):
        loads[name].wait()
    ti = lax.broadcasted_iota(jnp.int32, (rows, rows), 0)
    si = lax.broadcasted_iota(jnp.int32, (rows, rows), 1)
    lower = si <= ti
    cumul = lax.dot_general(
        r.ld[...],
        (ti <= si).astype(F32),
        (((1,), (0,)), ((), ())),
        precision=lax.Precision.HIGHEST,
        preferred_element_type=F32,
    )
    half = hd // 2
    lane = lax.broadcasted_iota(jnp.int32, (1, hd), 1)
    low_half = lane < half
    index = jnp.where(low_half, lane, lane - half).astype(F32)
    freq = jnp.exp(index * (-math.log(10000.0) / (half - 1)))
    angles = (sp * rows + lax.broadcasted_iota(jnp.int32, (rows, hd), 0)).astype(F32) * freq
    cos = jnp.cos(angles)
    sin = jnp.sin(angles)
    sin = jnp.where(low_half, -sin, sin)
    for h in range(heads):
        cols = slice(h * hd, (h + 1) * hd)
        qf = r.q[:, cols].astype(F32)
        kf = r.k[:, cols].astype(F32)
        vb = r.v[:, cols]
        qb = (qf * cos + pltpu.roll(qf, half, 1) * sin).astype(BF16)
        kb = ((kf * cos + pltpu.roll(kf, half, 1) * sin) * hd ** (-0.5)).astype(BF16)
        along = jnp.broadcast_to(cumul[h : h + 1, :], (rows, rows))
        cum = jnp.transpose(along)
        spread = cum - along
        weight_ts = jnp.where(lower, jnp.exp(jnp.where(lower, spread, 0.0)), 0.0)
        probs = (dot_nt(qb, kb) * weight_ts).astype(BF16)
        r.inner[:, cols] = dot_nn(probs, vb)
        last = cum[rows - 1 :, :]
        kw = kb.astype(F32) * jnp.exp(last - cum)
        r.c_out[h] = dot_nn(jnp.transpose(kw).astype(BF16), vb).astype(BF16)
        r.t_out[h] = jnp.broadcast_to(jnp.exp(last), r.t_out.shape[1:])
        r.qrot[:, cols] = qb
        r.cumx[:, cols] = jnp.exp(cum)

    my_h, its_h = pl.ds(x * hh, hh), pl.ds((1 - x) * hh, hh)
    x_one, c_one = dev(z, 1 - x, y, 1), dev(z, x, y, 1)

    def cross_c(k):
        return lambda: remote(
            r.c_out.at[its_h], r.ci.at[1, k], r.cx_send.at[0], r.cx_recv.at[0, k], x_one
        )

    def cross_t(k):
        return lambda: remote(
            r.t_out.at[its_h], r.ti.at[1, k], r.cx_send.at[1], r.cx_recv.at[1, k], x_one
        )

    go(cross_c(c))
    go(cross_t(c))

    def near_c():
        return remote(r.c_out.at[my_h], r.ci.at[0, 0], r.cc_send.at[0], r.cc_recv.at[0], c_one)

    def near_t():
        return remote(r.t_out.at[my_h], r.ti.at[0, 0], r.cc_send.at[1], r.cc_recv.at[1], c_one)

    def chain():
        up = jnp.minimum(z + 1, nz - 1)
        return remote(r.ch_out, r.ch_in, r.ch_send, r.ch_recv, dev(up, x, y, 1))

    def state_x(k):
        return lambda: remote(
            r.so.at[1, k], r.s_in.at[1], r.so_send.at[k], r.s_recv.at[1], dev(z, 1 - x, y, k)
        )

    def state_c():
        return remote(
            r.so.at[0, 0], r.s_in.at[0], r.so_send.at[2], r.s_recv.at[0], dev(z, x, y, 0)
        )

    @pl.when(c == 0)
    def _():
        go(near_c)
        go(near_t)
        for m in range(3):
            hand(m)().wait_recv()

        @pl.when(outer)
        def _():
            send_weights(outer_head, (1,))
            send_weights(outer_tail)

        @pl.when(jnp.logical_not(outer))
        def _():
            send_weights(inner_head, (1,))
            send_weights(inner_tail)

    late = z >= nz // 2
    first = x == 0

    def pass_own(when):
        @pl.when(when)
        def _():
            for m in range(2):
                forward(m, 0)().start()

    pass_own(late)

    @pl.when(c == 1)
    def _():
        r.ci[0, 1] = r.c_out[my_h]
        r.ti[0, 1] = r.t_out[my_h]
        near_c().wait_recv()
        near_t().wait_recv()
        for k in range(CS):
            cross_c(k)().wait_recv()
            cross_t(k)().wait_recv()
        for k in range(CS):
            for i in range(hh):
                own_c, own_t = r.ci[0, k, i].astype(F32), r.ti[0, k, i][:1]
                other_c, other_t = r.ci[1, k, i].astype(F32), r.ti[1, k, i][:1]
                early_c = jnp.where(first, own_c, other_c)
                late_c = jnp.where(first, other_c, own_c)
                late_t = jnp.where(first, other_t, own_t)
                r.plane[k, i] = late_t * early_c + late_c

        pass_if(late, near)

        @pl.when(z == 0)
        def _():
            r.ch_in[...] = jnp.zeros(r.ch_in.shape, BF16)

        @pl.when(z > 0)
        def _():
            chain().wait_recv()

        for k in range(CS):
            for i in range(hh):
                both_t = r.ti[0, k, i][:1] * r.ti[1, k, i][:1]
                state = r.ch_in[k, i].astype(F32)
                r.ch_out[k, i] = (both_t * state + r.plane[k, i]).astype(BF16)

        @pl.when(z < nz - 1)
        def _():
            go(chain)

        for k in range(CS):
            for i in range(hh):
                early_c = jnp.where(first, r.ci[0, k, i], r.ci[1, k, i]).astype(F32)
                early_t = jnp.where(first, r.ti[0, k, i][:1], r.ti[1, k, i][:1])
                state = r.ch_in[k, i].astype(F32)
                after = early_t * state + early_c
                r.so[0, k, i] = jnp.where(first, state, after).astype(BF16)
                r.so[1, k, i] = jnp.where(first, after, state).astype(BF16)
        for k in range(CS):
            go(state_x(k))
        go(state_c)
        r.s_in[0] = r.so[0, 1]

    @pl.when(c == 0)
    def _():
        pass_if(late, near)
        state_c().wait_recv()

    pass_own(jnp.logical_not(late))
    state_x(0)().wait_recv()
    loads["g"].wait()
    loads["hg"].wait()
    for h in range(heads):
        cols = slice(h * hd, (h + 1) * hd)
        state = r.s_in[lax.rem(x + h // hh, XS), h % hh]
        ret = r.inner[:, cols] + r.cumx[:, cols] * dot_nn(r.qrot[:, cols], state)
        scale = lax.rsqrt(jnp.mean(ret * ret, axis=-1, keepdims=True) + EPS)
        gf = r.g[:, cols].astype(F32)
        r.retained[:, cols] = (
            ret * scale * r.hg[:, cols] * (gf / (1.0 + jnp.exp(-gf)))
        ).astype(BF16)
    loads["ow"].wait()

    def mix_c():
        return remote(r.mc_out, r.mc_in, r.mix_send.at[0], r.mix_recv.at[0], c_peer)

    def mix_y():
        return remote(
            r.my_out, r.my_in, r.mix_send.at[1], r.mix_recv.at[1], dev(z, x, 1 - y, c)
        )

    def mix_part(cc):
        picked = [
            r.retained[pl.ds(pl.multiple_of((yy * CS + cc) * quarter, quarter), quarter), :]
            for yy in range(nt // CS)
        ]
        part = dot_nn(jnp.concatenate(picked, axis=0), r.ow[...])
        return part.reshape(nt // CS, quarter, part.shape[1])

    r.mc_out[...] = mix_part(1 - c).astype(BF16)
    go(mix_c)
    r.mix_own[...] = mix_part(c)
    mix_c().wait_recv()
    r.my_out[...] = (r.mix_own[1 - y] + r.mc_in[1 - y].astype(F32)).astype(BF16)
    go(mix_y)
    early = jnp.logical_not(late)
    pass_if(early, near)
    pass_on(0, 2)
    pass_if(late, ((0, 3),))
    mixed = r.mix_own[y] + r.mc_in[y].astype(F32)
    mix_y().wait_recv()
    mixed += r.my_in[...].astype(F32)
    loads["res"].wait()
    loads["mg"].wait()
    mid = (r.res[...].astype(F32) + mixed).astype(BF16).astype(F32)
    for g in range(nz):
        for u in range(XS):
            at = g * group + u * width
            r.acc[g, u] = mid[:, at : at + width]
    r.normed[z, tp] = (
        mid * lax.rsqrt(jnp.mean(mid * mid, axis=-1, keepdims=True) + EPS) * r.mg[...]
    ).astype(BF16)

    def rows_c():
        rows_at = r.normed.at[z, tp]
        return remote(rows_at, rows_at, r.nc_send, r.nc_recv, c_peer)

    def rows_of(zz, yy, j):
        return r.normed.at[zz, yy * CS + j]

    def rows_z(k, j):
        to = zat[2] if k == 0 else zat[1]
        zz = zat[2] if k == 2 else z
        return lambda: remote(
            rows_of(zz, y, j),
            rows_of(zz, y, j),
            r.nz_send,
            r.nz_recv.at[k, j],
            dev(to, x, y, 1),
        )

    def rows_y(e, j):
        return lambda: remote(
            rows_of(zat[e], y, j),
            rows_of(zat[e], y, j),
            r.ny_send,
            r.ny_recv.at[e, j],
            dev(z, x, 1 - y, 1),
        )

    def rows_d(e, v, j):
        def build():
            rows_at = rows_of(zat[e], 1 - y if v else y, j)
            return remote(
                rows_at, rows_at, r.nd_send.at[v], r.nd_recv.at[v, e], dev(z, x, y, 0)
            )

        return build

    def got_rows(e, v):
        view = r.normed.at[zat[e], pl.ds((1 - y if v else y) * CS, CS)]
        remote(view, view, r.nd_send.at[v], r.nd_recv.at[v, e], c_peer).wait_recv()

    go(rows_c)

    def send_down(if_outer, if_inner):
        @pl.when(outer)
        def _():
            send_weights(((2, if_outer),))

        @pl.when(jnp.logical_not(outer))
        def _():
            send_weights(((2, if_inner),))

    @pl.when(c == 1)
    def _():
        go(rows_z(0, 1))
        go(rows_y(0, 1))
        rows_c().wait_recv()
        go(rows_z(0, 0))
        for j in (1, 0):
            go(rows_z(1, j))
        go(rows_y(0, 0))

    @pl.when(c == 0)
    def _():
        rows_c().wait_recv()

    pass_if(early, ((0, 3),))
    own_copies[2].wait()
    pass_on(2, 0)
    pass_on(1, 3)

    @pl.when(c == 1)
    def _():
        for j in (1, 0):
            rows_z(1, j)().wait_recv()
            go(rows_y(1, j))
            go(rows_d(1, 0, j))
        for j in (1, 0):
            rows_y(0, j)().wait_recv()
            go(rows_d(0, 1, j))
        for j in (1, 0):
            rows_z(0, j)().wait_recv()
            go(rows_z(2, j))
            go(rows_y(2, j))
            go(rows_d(2, 0, j))

    pass_on(1, 2)
    pass_on(2, 1)

    @pl.when(c == 0)
    def _():
        got_rows(2, 0)
        send_down(2, 3)

    @pl.when(c == 1)
    def _():
        for j in (1, 0):
            rows_y(1, j)().wait_recv()
            go(rows_d(1, 1, j))
        for j in (1, 0):
            rows_z(2, j)().wait_recv()
            go(rows_y(3, j))
            go(rows_d(3, 0, j))

    @pl.when(c == 0)
    def _():
        got_rows(3, 0)
        send_down(3, 2)
        for e, v in ((1, 0), (0, 1), (1, 1)):
            got_rows(e, v)

    def project(m, half_z):
        block = r.normed[pl.ds(2 * half_z, 2)].reshape(2 * rows, r.normed.shape[3])
        total = dot_nt(block[:, :width], r.wg[m, 0])
        for s in range(1, ns):
            total += dot_nt(block[:, s * width : (s + 1) * width], r.wg[m, s])
        return total

    def gate_rows(half_z):
        gate = project(0, half_z)
        r.gated[half_z] = gate / (1.0 + jnp.exp(-gate))

    def half_at(half_z):
        return pl.ds(pl.multiple_of(half_z * 2 * rows, 2 * rows), 2 * rows)

    def hand_hidden(i):
        at = half_at(own_half if i == 0 else 1 - own_half)
        return lambda: remote(
            r.hidden.at[0, at], r.hidden.at[1, at], r.hx_send, r.hx_recv.at[i], x_peer
        )

    def up_rows(i):
        half_z = own_half if i == 0 else 1 - own_half
        r.hidden[0, half_at(half_z), :] = (r.gated[half_z] * project(1, half_z)).astype(BF16)
        go(hand_hidden(i))

    own_half = z // 2
    own_copies[0].wait()
    got_forwards(0)
    gate_rows(own_half)

    @pl.when(c == 1)
    def _():
        for e in (2, 3):
            for j in (1, 0):
                rows_y(e, j)().wait_recv()
                go(rows_d(e, 1, j))

    own_copies[1].wait()
    got_forwards(1)
    up_rows(0)

    @pl.when(c == 0)
    def _():
        for e in (2, 3):
            got_rows(e, 1)

    gate_rows(1 - own_half)
    up_rows(1)

    low = c == 0

    def t1(b, u):
        return lambda: remote(
            r.s1.at[b, u], r.r1.at[b, u], r.t1_send, r.t1_recv.at[b, u], c_peer
        )

    def t2(b, u):
        return lambda: remote(
            r.s2.at[b, u],
            r.r2.at[b, u],
            r.t2_send,
            r.t2_recv.at[b, u],
            dev(z, x, 1 - y, c),
        )

    def unit(b, u):
        return XS * b + u if b < 2 else b + 2

    def t3(b, u, e):
        if b > 1 and u:
            return lambda: remote(
                r.s3x.at[b - 2, e],
                r.r3x.at[b - 2, e],
                r.t3x_send,
                r.t3x_recv.at[b - 2],
                dev(zat[e], 1 - x, y, c),
            )
        return lambda: remote(
            r.s3.at[unit(b, u), e - 1],
            r.r3.at[unit(b, u), e - 1],
            r.t3_send,
            r.t3_recv.at[unit(b, u)],
            dev(zat[e], x, y, c),
        )

    def side(u):
        return 1 - x if u else x

    def compute(b, u):
        if b < 2:
            if u:
                forward(2, b)().wait_recv()
            part = dot_nn(r.hidden[0], r.wg[2, zat[b] * XS + side(u)])
        else:
            part = dot_nn(r.hidden[u], r.wg[2, zat[b] * XS + x])
        for zz in range(nz):
            for yy in range(nt // CS):
                at = zz * rows + yy * CS * quarter
                even = part[at : at + quarter]
                odd = part[at + quarter : at + 2 * quarter]
                r.keep[b, u, yy, zz] = jnp.where(low, even, odd)
                r.s1[b, u, yy, zz] = jnp.where(low, odd, even).astype(BF16)
        go(t1(b, u))

    def second(b, u):
        t1(b, u)().wait_recv()
        r.s2[b, u] = (r.keep[b, u, 1 - y] + r.r1[b, u, 1 - y].astype(F32)).astype(BF16)
        go(t2(b, u))
        r.keep[b, u, y] = r.keep[b, u, y] + r.r1[b, u, y].astype(F32)

    def third(b, u):
        t2(b, u)().wait_recv()
        def value(e):
            return r.keep[b, u, y, zat[e]] + r.r2[b, u, zat[e]].astype(F32)

        if b > 1 and u:
            for e in (3, 2, 1, 0):
                r.s3x[b - 2, e] = value(e).astype(BF16)
                go(t3(b, u, e))
            return
        for e in (3, 2, 1):
            r.s3[unit(b, u), e - 1] = value(e).astype(BF16)
            go(t3(b, u, e))
        r.acc[zat[b], side(u)] = r.acc[zat[b], side(u)] + value(0)

    def last(b, u):
        if b > 1 and u:
            view = r.r3x.at[b - 2]
            remote(view, view, r.t3x_send, r.t3x_recv.at[b - 2], c_peer).wait_recv()
            for e in range(nz):
                g = zat[b ^ e]
                r.acc[g, 1 - x] = r.acc[g, 1 - x] + r.r3x[b - 2, e].astype(F32)
            return
        view = r.r3.at[unit(b, u)]
        remote(view, view, r.t3_send, r.t3_recv.at[unit(b, u)], c_peer).wait_recv()
        for e in (1, 3, 2):
            g = zat[b ^ e]
            r.acc[g, side(u)] = r.acc[g, side(u)] + r.r3[unit(b, u), e - 1].astype(F32)

    def other_hidden():
        for i in range(2):
            hand_hidden(i)().wait_recv()

    for b in range(2):
        for u in range(XS):
            compute(b, u)
    for b in range(2):
        for u in range(XS):
            second(b, u)
    got_weight(2, 3)
    compute(3, 0)
    third(0, 0)
    second(3, 0)
    third(0, 1)
    got_weight(2, 2)
    compute(2, 0)
    other_hidden()
    compute(3, 1)
    compute(2, 1)
    third(1, 0)
    second(2, 0)
    second(3, 1)
    second(2, 1)
    third(1, 1)
    third(3, 0)
    third(2, 0)
    third(3, 1)
    third(2, 1)
    for b in (0, 1):
        for u in range(XS):
            last(b, u)
    for b, u in ((3, 0), (2, 0), (3, 1), (2, 1)):
        last(b, u)
    for g in range(nz):
        for u in range(XS):
            at = g * group + u * width
            r.out[:, at : at + width] = r.acc[g, u].astype(BF16)

    sent(r.wg.at[:2, : nz + 1], r.f_send)
    sent(r.hidden.at[0], r.hx_send)
    sent(r.s1, r.t1_send)
    sent(r.s2, r.t2_send)
    sent(r.s3, r.t3_send)
    sent(r.s3x, r.t3x_send)
    for build in (cross_c(c), cross_t(c), rows_c, mix_c, mix_y):
        build().wait_send()

    @pl.when(c == 0)
    def _():
        sent(r.wg.at[:, : CS * (nz - 1)], r.w_send)
        near_c().wait_send()
        near_t().wait_send()

    @pl.when(c == 1)
    def _():
        sent(r.slab, r.h_send)
        sent(r.normed.at[:3, :CS], r.nz_send)
        sent(r.normed.at[:CS], r.ny_send)
        sent(r.normed.at[: nz - 1, :CS], r.nd_send.at[0])
        sent(r.normed.at[:CS], r.nd_send.at[1])
        for build in (state_x(0), state_x(1), state_c):
            build().wait_send()

    @pl.when(jnp.logical_and(c == 1, z < nz - 1))
    def _():
        chain().wait_send()


def fast_body(
    queries,
    key_rows,
    value_rows,
    gate_input,
    log_decay,
    head_gain,
    out_weight,
    residual,
    mlp_gain,
    gate_weight,
    up_weight,
    down_weight,
):
    rows, wide = queries.shape
    heads = log_decay.shape[1]
    hd = wide // heads
    model = residual.shape[1]
    ns, nt = lax.axis_size("sp"), lax.axis_size("tp")
    nz = ns // XS
    quarter = rows // nt
    width, units = gate_weight.shape
    share = units // nz
    hh = heads // XS
    vmem = pltpu.VMEM
    dma = pltpu.SemaphoreType.DMA
    operands = {
        "q_hbm": queries,
        "k_hbm": key_rows,
        "v_hbm": value_rows,
        "g_hbm": gate_input,
        "ld_hbm": log_decay.T,
        "hg_hbm": head_gain.reshape(1, wide),
        "res_hbm": residual,
        "mg_hbm": mlp_gain.reshape(1, model),
        "ow_hbm": out_weight,
        "gw_hbm": gate_weight,
        "uw_hbm": up_weight,
        "dw_hbm": down_weight,
    }
    scratch = {
        "q": vmem((rows, wide), BF16),
        "k": vmem((rows, wide), BF16),
        "v": vmem((rows, wide), BF16),
        "g": vmem((rows, wide), BF16),
        "ld": vmem((heads, rows), F32),
        "hg": vmem((1, wide), F32),
        "res": vmem((quarter, model), BF16),
        "mg": vmem((1, model), F32),
        "ow": vmem(out_weight.shape, BF16),
        "raw": vmem((2, width, units), BF16),
        "slab": vmem((3, units, width), BF16),
        "partner": vmem((3, units, width), BF16),
        "wg": vmem((3, ns, share, width), BF16),
        "qrot": vmem((rows, wide), BF16),
        "inner": vmem((rows, wide), F32),
        "cumx": vmem((rows, wide), F32),
        "c_out": vmem((heads, hd, hd), BF16),
        "t_out": vmem((heads, 8, hd), F32),
        "ci": vmem((XS, CS, hh, hd, hd), BF16),
        "ti": vmem((XS, CS, hh, 8, hd), F32),
        "plane": vmem((CS, hh, hd, hd), F32),
        "ch_in": vmem((CS, hh, hd, hd), BF16),
        "ch_out": vmem((CS, hh, hd, hd), BF16),
        "so": vmem((XS, CS, hh, hd, hd), BF16),
        "s_in": vmem((XS, hh, hd, hd), BF16),
        "retained": vmem((rows, wide), BF16),
        "mc_out": vmem((nt // CS, quarter, model), BF16),
        "mc_in": vmem((nt // CS, quarter, model), BF16),
        "mix_own": vmem((nt // CS, quarter, model), F32),
        "my_out": vmem((quarter, model), BF16),
        "my_in": vmem((quarter, model), BF16),
        "acc": vmem((nz, XS, quarter, width), F32),
        "normed": vmem((nz, nt, quarter, model), BF16),
        "gated": vmem((nz // 2, 2 * rows, share), F32),
        "hidden": vmem((XS, nz * rows, share), BF16),
        "keep": vmem((nz, XS, nt // CS, nz, quarter, width), F32),
        "s1": vmem((nz, XS, nt // CS, nz, quarter, width), BF16),
        "r1": vmem((nz, XS, nt // CS, nz, quarter, width), BF16),
        "s2": vmem((nz, XS, nz, quarter, width), BF16),
        "r2": vmem((nz, XS, nz, quarter, width), BF16),
        "s3": vmem((nz + 2, nz - 1, quarter, width), BF16),
        "r3": vmem((nz + 2, nz - 1, quarter, width), BF16),
        "s3x": vmem((2, nz, quarter, width), BF16),
        "r3x": vmem((2, nz, quarter, width), BF16),
        "in_sem": dma((len(operands),)),
        "own_sem": dma((3,)),
        "h_send": dma,
        "h_recv": dma((3,)),
        "w_send": dma,
        "w_recv": dma((3, nz - 1)),
        "f_send": dma,
        "f_recv": dma((4,)),
        "cx_send": dma((2,)),
        "cx_recv": dma((2, CS)),
        "cc_send": dma((2,)),
        "cc_recv": dma((2,)),
        "ch_send": dma,
        "ch_recv": dma,
        "so_send": dma((3,)),
        "s_recv": dma((XS,)),
        "mix_send": dma((2,)),
        "mix_recv": dma((2,)),
        "nc_send": dma,
        "nc_recv": dma,
        "nz_send": dma,
        "nz_recv": dma((3, CS)),
        "ny_send": dma,
        "ny_recv": dma((nz, CS)),
        "nd_send": dma((2,)),
        "nd_recv": dma((2, nz)),
        "t1_send": dma,
        "t1_recv": dma((nz, XS)),
        "t2_send": dma,
        "t2_recv": dma((nz, XS)),
        "t3_send": dma,
        "t3_recv": dma((nz + 2,)),
        "t3x_send": dma,
        "t3x_recv": dma((2,)),
        "hx_send": dma,
        "hx_recv": dma((2,)),
    }
    names = list(operands) + ["out"] + list(scratch)
    return pl.pallas_call(
        functools.partial(kernel, names, nz, nt),
        out_shape=pltpu.VMEM((quarter, model), BF16),
        in_specs=[pl.BlockSpec(memory_space=pl.ANY)] * len(operands),
        out_specs=pl.BlockSpec(memory_space=pltpu.VMEM),
        scratch_shapes=list(scratch.values()),
        compiler_params=pltpu.CompilerParams(
            collective_id=0, has_side_effects=True, vmem_limit_bytes=60 * 1024 * 1024
        ),
    )(*operands.values())


def fits(mesh, queries, log_decay, gate_weight):
    ns, nt = mesh.shape["sp"], mesh.shape["tp"]
    tokens, wide = queries.shape
    if ns % XS or ns // XS != 4 or nt != 2 * CS or tokens // ns != BLOCK:
        return False
    nz = ns // XS
    hidden = gate_weight.shape[1] // nt
    return (
        gate_weight.shape[0] // ns % 128 == 0
        and hidden % (16 * nz) == 0
        and wide // log_decay.shape[1] == 128
        and BLOCK % (16 * nt) == 0
        and hidden % 128 == 0
        and log_decay.shape[1] // nt % XS == 0
    )


def solution(mesh):
    def run(*args):
        good = fits(mesh, args[0], args[4], args[9])
        return jax.shard_map(
            fast_body if good else body,
            mesh=mesh,
            in_specs=(
                P("sp", "tp"),
                P("sp", "tp"),
                P("sp", "tp"),
                P("sp", "tp"),
                P("sp", "tp"),
                P("tp"),
                P("tp", None),
                P("sp", None),
                P(),
                P("sp", "tp"),
                P("sp", "tp"),
                P("tp", "sp"),
            ),
            out_specs=P(("sp", "tp"), None),
            check_vma=False,
        )(*args)

    return run
```

```python
import functools
import math
import types

import jax
import jax.numpy as jnp
from jax import lax
from jax.experimental import pallas as pl
from jax.experimental.pallas import tpu as pltpu
from jax.sharding import PartitionSpec as P

BLOCK = 128


EPS = 1e-06


def prefix_2(x, axis, join, neutral):
    place = lax.axis_index(axis)
    gathered = jax.tree.map(
        lambda a, kind: lax.all_gather(a.astype(kind), axis), x, (jnp.bfloat16, jnp.bfloat16)
    )
    state = jax.tree.map(lambda a, e: jnp.zeros_like(a) + jnp.asarray(e, a.dtype), x, neutral)

    def one(step, state):
        return join(
            state,
            jax.tree.map(
                lambda a, own: lax.dynamic_index_in_dim(a, step, 0, False).astype(own.dtype),
                gathered,
                x,
            ),
        )

    return lax.fori_loop(0, place, one, state)


def rotate(values_in, positions):
    half = values_in.shape[-1] // 2
    freq = 10000.0 ** (-jnp.linspace(0.0, 1.0, half, dtype=jnp.float32))
    angles = positions * freq
    angles = jnp.concatenate([angles, angles], axis=-1)
    first = values_in[..., :half]
    second = values_in[..., half:]
    turned = jnp.concatenate([-second, first], axis=-1)
    return values_in * jnp.cos(angles) + turned * jnp.sin(angles)


def row_norm(stream, gain):
    return stream * lax.rsqrt(jnp.mean(stream * stream, axis=-1, keepdims=True) + EPS) * gain


def join_states(earlier, later):
    return (earlier[0] * later[0], later[0][:, None, None] * earlier[1] + later[1])


def body(
    queries,
    key_rows,
    value_rows,
    gate_input,
    log_decay,
    head_gain,
    out_weight,
    residual,
    mlp_gain,
    gate_weight,
    up_weight,
    down_weight,
):
    tok_rows = queries.shape[0]
    heads_here = log_decay.shape[1]
    head_size = head_gain.shape[0] // heads_here
    quarter = tok_rows // lax.axis_size("tp")
    offset = lax.axis_index("sp") * tok_rows
    positions = (offset + lax.iota(jnp.int32, tok_rows)).astype(jnp.float32)[:, None, None]
    q_rot = rotate(
        queries.reshape(tok_rows, heads_here, head_size).astype(jnp.float32), positions
    ).astype(jnp.bfloat16)
    k_rot = (
        rotate(key_rows.reshape(tok_rows, heads_here, head_size).astype(jnp.float32), positions)
        * head_size ** (-0.5)
    ).astype(jnp.bfloat16)
    blocks = tok_rows // BLOCK
    q_blocks = q_rot.reshape(blocks, BLOCK, heads_here, head_size)
    k_blocks = k_rot.reshape(blocks, BLOCK, heads_here, head_size)
    v_blocks = value_rows.reshape(blocks, BLOCK, heads_here, head_size)
    cumul = jnp.cumsum(log_decay.reshape(blocks, BLOCK, heads_here), axis=1)
    by_head = cumul.transpose(0, 2, 1)
    lower = jnp.tril(jnp.ones((BLOCK, BLOCK), dtype=bool))
    spread = by_head[:, :, :, None] - by_head[:, :, None, :]
    weight = jnp.where(lower, jnp.exp(jnp.where(lower, spread, 0.0)), 0.0)
    scores = jnp.einsum("nthd,nshd->nhts", q_blocks, k_blocks, preferred_element_type=jnp.float32)
    probs = (scores * weight).astype(jnp.bfloat16)
    inner = jnp.einsum("nhts,nshe->nthe", probs, v_blocks, preferred_element_type=jnp.float32)
    k_weighted = (
        k_blocks.astype(jnp.float32) * jnp.exp(cumul[:, -1:, :] - cumul)[..., None]
    ).astype(jnp.bfloat16)
    contrib = jnp.einsum(
        "nshd,nshe->nhde", k_weighted, v_blocks, preferred_element_type=jnp.float32
    )
    totals = jnp.exp(cumul[:, -1, :])

    def advance(carry, items):
        state, prefix = carry
        factor, update = items
        return ((state * factor[:, None, None] + update, prefix * factor), (state, prefix))

    start_state = jnp.zeros((heads_here, head_size, head_size), jnp.float32)
    start_prefix = jnp.ones((heads_here,), jnp.float32)
    (dev_state, dev_total), (local_before, prefixes) = lax.scan(
        advance, (start_state, start_prefix), (totals, contrib)
    )
    _, incoming = prefix_2((dev_total, dev_state), "sp", join_states, (start_prefix, start_state))
    before = local_before + prefixes[:, :, None, None] * incoming[None]
    cross = jnp.einsum(
        "nthd,nhde->nthe", q_blocks.astype(jnp.float32), before, precision=lax.Precision.HIGHEST
    )
    cross = cross * jnp.exp(cumul)[..., None]
    result = (inner + cross).reshape(tok_rows, heads_here, head_size)
    result = row_norm(result, head_gain.reshape(heads_here, head_size)).reshape(
        tok_rows, heads_here * head_size
    )
    retained = (result * jax.nn.silu(gate_input.astype(jnp.float32))).astype(jnp.bfloat16)
    picked = retained
    mixed = lax.psum_scatter(
        jnp.dot(picked, out_weight, preferred_element_type=jnp.float32).astype(jnp.bfloat16),
        "tp",
        scatter_dimension=0,
        tiled=True,
    ).astype(jnp.float32)
    own_rows = lax.dynamic_slice_in_dim(residual, lax.axis_index("tp") * quarter, quarter, 0)
    rows_mid = (own_rows.astype(jnp.float32) + mixed).astype(jnp.bfloat16)
    own_normed = row_norm(rows_mid.astype(jnp.float32), mlp_gain).astype(jnp.bfloat16)
    normed = lax.all_gather(own_normed, "tp", axis=0, tiled=True)
    gate = jnp.dot(
        normed,
        lax.all_gather(gate_weight, "sp", axis=0, tiled=True),
        preferred_element_type=jnp.float32,
    )
    upvals = jnp.dot(
        normed,
        lax.all_gather(up_weight, "sp", axis=0, tiled=True),
        preferred_element_type=jnp.float32,
    )
    full_down = lax.all_gather(down_weight, "sp", axis=1, tiled=True)
    hidden = (jax.nn.silu(gate) * upvals).astype(jnp.bfloat16)
    picked = hidden
    ffn = lax.psum_scatter(
        jnp.dot(picked, full_down, preferred_element_type=jnp.float32).astype(jnp.bfloat16),
        "tp",
        scatter_dimension=0,
        tiled=True,
    ).astype(jnp.float32)
    return (rows_mid.astype(jnp.float32) + ffn).astype(jnp.bfloat16)


MESH = pl.DeviceIdType.MESH
XS = 2
CS = 2
F32 = jnp.float32
BF16 = jnp.bfloat16


def dot_nt(a, b):
    return lax.dot_general(a, b, (((1,), (1,)), ((), ())), preferred_element_type=F32)


def dot_nn(a, b):
    return lax.dot_general(a, b, (((1,), (0,)), ((), ())), preferred_element_type=F32)


def kernel(names, nz, nt, *refs):
    r = types.SimpleNamespace(**dict(zip(names, refs)))
    sp = lax.axis_index("sp")
    tp = lax.axis_index("tp")
    z, x = sp // XS, lax.rem(sp, XS)
    y, c = tp // CS, lax.rem(tp, CS)
    rows = r.q.shape[0]
    heads = r.ld.shape[0]
    hh = heads // XS
    hd = r.q.shape[1] // heads
    quarter = rows // nt
    share, width = r.wg.shape[2], r.wg.shape[3]
    group = XS * width
    ns = nz * XS
    zat = [z, z + 1 - 2 * lax.rem(z, 2), lax.rem(z + 2, nz), nz - 1 - z]

    def dev(zz, xx, yy, cc):
        return (zz * XS + xx, yy * CS + cc)

    x_peer = dev(z, 1 - x, y, c)
    c_peer = dev(z, x, y, 1 - c)

    barrier = pltpu.get_barrier_semaphore()
    peers = [dev(zat[e], x, y, k) for e in range(1, nz) for k in range(CS)]
    peers += [c_peer] + [dev(zat[e], 1 - x, y, c) for e in range(1, nz)]
    peers += [dev(z, 1 - x, y, k) for k in range(CS)]
    peers += [dev(z, x, 1 - y, k) for k in range(CS)]
    for peer in peers:
        pl.semaphore_signal(barrier, inc=1, device_id=peer, device_id_type=MESH)

    loads = {}

    def load(name, src, dst):
        loads[name] = pltpu.make_async_copy(src, dst, r.in_sem.at[len(loads)])
        loads[name].start()

    load("gw", r.gw_hbm, r.raw.at[0])
    load("uw", r.uw_hbm, r.raw.at[1])
    for name in ("ld", "q", "k", "v"):
        load(name, getattr(r, name + "_hbm"), getattr(r, name))
    load("dw", r.dw_hbm, r.slab.at[2])
    for name in ("g", "hg", "ow", "mg"):
        load(name, getattr(r, name + "_hbm"), getattr(r, name))
    mine = pl.multiple_of(tp * quarter, quarter)
    load("res", r.res_hbm.at[pl.ds(mine, quarter)], r.res)

    def remote(src, dst, send, recv, peer):
        return pltpu.make_async_remote_copy(
            src_ref=src,
            dst_ref=dst,
            send_sem=send,
            recv_sem=recv,
            device_id=peer,
            device_id_type=MESH,
        )

    def go(build):
        build().start()

    def sent(view, sem):
        remote(view, view, sem, sem, c_peer).wait_send()

    def piece(ref, m, zz):
        return ref.at[m, pl.ds(pl.multiple_of(zz * share, 16), share)]

    def slot(m, zz):
        return r.wg.at[m, zz * XS + x]

    own_copies = {}

    def take_own(m):
        own_copies[m] = pltpu.make_async_copy(piece(r.slab, m, z), slot(m, z), r.own_sem.at[m])
        own_copies[m].start()

    for m, name in enumerate(("gw", "uw")):
        loads[name].wait()
        for j in range(r.raw.shape[2] // 128):
            r.slab[m, j * 128 : (j + 1) * 128, :] = jnp.transpose(
                r.raw[m, :, j * 128 : (j + 1) * 128]
            )
        take_own(m)
    loads["dw"].wait()
    take_own(2)
    for name in ("ld", "q", "k", "v"):
        loads[name].wait()
    ti = lax.broadcasted_iota(jnp.int32, (rows, rows), 0)
    si = lax.broadcasted_iota(jnp.int32, (rows, rows), 1)
    lower = si <= ti
    cumul = lax.dot_general(
        r.ld[...],
        (ti <= si).astype(F32),
        (((1,), (0,)), ((), ())),
        precision=lax.Precision.HIGHEST,
        preferred_element_type=F32,
    )
    half = hd // 2
    lane = lax.broadcasted_iota(jnp.int32, (1, hd), 1)
    low_half = lane < half
    index = jnp.where(low_half, lane, lane - half).astype(F32)
    freq = jnp.exp(index * (-math.log(10000.0) / (half - 1)))
    angles = (sp * rows + lax.broadcasted_iota(jnp.int32, (rows, hd), 0)).astype(F32) * freq
    cos = jnp.cos(angles)
    sin = jnp.sin(angles)
    sin = jnp.where(low_half, -sin, sin)
    for h in range(heads):
        cols = slice(h * hd, (h + 1) * hd)
        qf = r.q[:, cols].astype(F32)
        kf = r.k[:, cols].astype(F32)
        vb = r.v[:, cols]
        qb = (qf * cos + pltpu.roll(qf, half, 1) * sin).astype(BF16)
        kb = ((kf * cos + pltpu.roll(kf, half, 1) * sin) * hd ** (-0.5)).astype(BF16)
        along = jnp.broadcast_to(cumul[h : h + 1, :], (rows, rows))
        cum = jnp.transpose(along)
        spread = cum - along
        weight_ts = jnp.where(lower, jnp.exp(jnp.where(lower, spread, 0.0)), 0.0)
        probs = (dot_nt(qb, kb) * weight_ts).astype(BF16)
        r.inner[:, cols] = dot_nn(probs, vb)
        last = cum[rows - 1 :, :]
        kw = kb.astype(F32) * jnp.exp(last - cum)
        r.c_out[h] = dot_nn(jnp.transpose(kw).astype(BF16), vb).astype(BF16)
        r.t_out[h] = jnp.broadcast_to(jnp.exp(last), r.t_out.shape[1:])
        r.qrot[:, cols] = qb
        r.cumx[:, cols] = jnp.exp(cum)

    pl.semaphore_wait(barrier, len(peers))

    def hand(m):
        return lambda: remote(
            r.slab.at[m], r.partner.at[m], r.h_send, r.h_recv.at[m], c_peer
        )

    def weight(m, e, k):
        source = r.partner if k else r.slab
        return lambda: remote(
            piece(source, m, zat[e]),
            slot(m, z),
            r.w_send,
            r.w_recv.at[m, e - 1],
            dev(zat[e], x, y, k),
        )

    outer = jnp.logical_or(z == 0, z == nz - 1)
    outer_head = ((0, 1), (1, 1))
    outer_tail = ((2, 1), (0, 2), (0, 3), (1, 2), (1, 3))
    inner_head = ((0, 3), (0, 1), (1, 3), (1, 1))
    inner_tail = ((2,1),(0,2),(1,2))

    def send_weights(plan, which=range(CS)):
        for m, e in plan:
            for k in which:
                weight(m, e, k)().start()

    def got_weight(m, e):
        weight(m, e, 0)().wait_recv()

    def forward(m, e):
        at = slot(m, zat[e])
        source = piece(r.slab, m, z) if e == 0 else at
        recv = r.f_recv.at[2 + e] if m == 2 else r.f_recv.at[m]
        return lambda: remote(source, at, r.f_send, recv, x_peer)

    def pass_on(m, e):
        if e:
            got_weight(m, e)
        go(forward(m, e))

    def pass_if(when, pieces):
        @pl.when(when)
        def _():
            for m, e in pieces:
                got_weight(m, e)
                forward(m, e)().start()

    near = ((0, 1), (1, 1))

    def got_forwards(m):
        view = r.wg.at[m, :nz]
        remote(view, view, r.f_send, r.f_recv.at[m], x_peer).wait_recv()

    @pl.when(c == 1)
    def _():
        for m in range(3):
            go(hand(m))

    @pl.when(jnp.logical_and(c == 0, outer))
    def _():
        send_weights(outer_head, (0,))

    @pl.when(jnp.logical_and(c == 0, jnp.logical_not(outer)))
    def _():
        send_weights(inner_head, (0,))

    my_h, its_h = pl.ds(x * hh, hh), pl.ds((1 - x) * hh, hh)
    x_one, c_one = dev(z, 1 - x, y, 1), dev(z, x, y, 1)

    def cross_c(k):
        return lambda: remote(
            r.c_out.at[its_h], r.ci.at[1, k], r.cx_send.at[0], r.cx_recv.at[0, k], x_one
        )

    def cross_t(k):
        return lambda: remote(
            r.t_out.at[its_h], r.ti.at[1, k], r.cx_send.at[1], r.cx_recv.at[1, k], x_one
        )

    go(cross_c(c))
    go(cross_t(c))

    def near_c():
        return remote(r.c_out.at[my_h], r.ci.at[0, 0], r.cc_send.at[0], r.cc_recv.at[0], c_one)

    def near_t():
        return remote(r.t_out.at[my_h], r.ti.at[0, 0], r.cc_send.at[1], r.cc_recv.at[1], c_one)

    def chain():
        up = jnp.minimum(z + 1, nz - 1)
        return remote(r.ch_out, r.ch_in, r.ch_send, r.ch_recv, dev(up, x, y, 1))

    def state_x(k):
        return lambda: remote(
            r.so.at[1, k], r.s_in.at[1], r.so_send.at[k], r.s_recv.at[1], dev(z, 1 - x, y, k)
        )

    def state_c():
        return remote(
            r.so.at[0, 0], r.s_in.at[0], r.so_send.at[2], r.s_recv.at[0], dev(z, x, y, 0)
        )

    @pl.when(c == 0)
    def _():
        go(near_c)
        go(near_t)
        for m in range(3):
            hand(m)().wait_recv()

        @pl.when(outer)
        def _():
            send_weights(outer_head, (1,))
            send_weights(outer_tail)

        @pl.when(jnp.logical_not(outer))
        def _():
            send_weights(inner_head, (1,))
            send_weights(inner_tail)

    late = z >= nz // 2
    first = x == 0

    def pass_own(when):
        @pl.when(when)
        def _():
            for m in range(2):
                forward(m, 0)().start()

    pass_own(late)

    @pl.when(c == 1)
    def _():
        r.ci[0, 1] = r.c_out[my_h]
        r.ti[0, 1] = r.t_out[my_h]
        near_c().wait_recv()
        near_t().wait_recv()
        for k in range(CS):
            cross_c(k)().wait_recv()
            cross_t(k)().wait_recv()
        for k in range(CS):
            for i in range(hh):
                own_c, own_t = r.ci[0, k, i].astype(F32), r.ti[0, k, i][:1]
                other_c, other_t = r.ci[1, k, i].astype(F32), r.ti[1, k, i][:1]
                early_c = jnp.where(first, own_c, other_c)
                late_c = jnp.where(first, other_c, own_c)
                late_t = jnp.where(first, other_t, own_t)
                r.plane[k, i] = late_t * early_c + late_c

        pass_if(late, near)

        @pl.when(z == 0)
        def _():
            r.ch_in[...] = jnp.zeros(r.ch_in.shape, BF16)

        @pl.when(z > 0)
        def _():
            chain().wait_recv()

        for k in range(CS):
            for i in range(hh):
                both_t = r.ti[0, k, i][:1] * r.ti[1, k, i][:1]
                state = r.ch_in[k, i].astype(F32)
                r.ch_out[k, i] = (both_t * state + r.plane[k, i]).astype(BF16)

        @pl.when(z < nz - 1)
        def _():
            go(chain)

        for k in range(CS):
            for i in range(hh):
                early_c = jnp.where(first, r.ci[0, k, i], r.ci[1, k, i]).astype(F32)
                early_t = jnp.where(first, r.ti[0, k, i][:1], r.ti[1, k, i][:1])
                state = r.ch_in[k, i].astype(F32)
                after = early_t * state + early_c
                r.so[0, k, i] = jnp.where(first, state, after).astype(BF16)
                r.so[1, k, i] = jnp.where(first, after, state).astype(BF16)
        for k in range(CS):
            go(state_x(k))
        go(state_c)
        r.s_in[0] = r.so[0, 1]

    @pl.when(c == 0)
    def _():
        pass_if(late, near)
        state_c().wait_recv()

    pass_own(jnp.logical_not(late))
    state_x(0)().wait_recv()
    loads["g"].wait()
    loads["hg"].wait()
    for h in range(heads):
        cols = slice(h * hd, (h + 1) * hd)
        state = r.s_in[lax.rem(x + h // hh, XS), h % hh]
        ret = r.inner[:, cols] + r.cumx[:, cols] * dot_nn(r.qrot[:, cols], state)
        scale = lax.rsqrt(jnp.mean(ret * ret, axis=-1, keepdims=True) + EPS)
        gf = r.g[:, cols].astype(F32)
        r.retained[:, cols] = (
            ret * scale * r.hg[:, cols] * (gf / (1.0 + jnp.exp(-gf)))
        ).astype(BF16)
    loads["ow"].wait()

    def mix_c():
        return remote(r.mc_out, r.mc_in, r.mix_send.at[0], r.mix_recv.at[0], c_peer)

    def mix_y():
        return remote(
            r.my_out, r.my_in, r.mix_send.at[1], r.mix_recv.at[1], dev(z, x, 1 - y, c)
        )

    def mix_part(cc):
        picked = [
            r.retained[pl.ds(pl.multiple_of((yy * CS + cc) * quarter, quarter), quarter), :]
            for yy in range(nt // CS)
        ]
        part = dot_nn(jnp.concatenate(picked, axis=0), r.ow[...])
        return part.reshape(nt // CS, quarter, part.shape[1])

    r.mc_out[...] = mix_part(1 - c).astype(BF16)
    go(mix_c)
    r.mix_own[...] = mix_part(c)
    mix_c().wait_recv()
    r.my_out[...] = (r.mix_own[1 - y] + r.mc_in[1 - y].astype(F32)).astype(BF16)
    go(mix_y)
    early = jnp.logical_not(late)
    pass_if(early, near)
    pass_on(0, 2)
    pass_if(late, ((0, 3),))
    mixed = r.mix_own[y] + r.mc_in[y].astype(F32)
    mix_y().wait_recv()
    mixed += r.my_in[...].astype(F32)
    loads["res"].wait()
    loads["mg"].wait()
    mid = (r.res[...].astype(F32) + mixed).astype(BF16).astype(F32)
    for g in range(nz):
        for u in range(XS):
            at = g * group + u * width
            r.acc[g, u] = mid[:, at : at + width]
    r.normed[z, tp] = (
        mid * lax.rsqrt(jnp.mean(mid * mid, axis=-1, keepdims=True) + EPS) * r.mg[...]
    ).astype(BF16)

    def rows_c():
        rows_at = r.normed.at[z, tp]
        return remote(rows_at, rows_at, r.nc_send, r.nc_recv, c_peer)

    def rows_of(zz, yy, j):
        return r.normed.at[zz, yy * CS + j]

    def rows_z(k, j):
        to = zat[2] if k == 0 else zat[1]
        zz = zat[2] if k == 2 else z
        return lambda: remote(
            rows_of(zz, y, j),
            rows_of(zz, y, j),
            r.nz_send,
            r.nz_recv.at[k, j],
            dev(to, x, y, 1),
        )

    def rows_y(e, j):
        return lambda: remote(
            rows_of(zat[e], y, j),
            rows_of(zat[e], y, j),
            r.ny_send,
            r.ny_recv.at[e, j],
            dev(z, x, 1 - y, 1),
        )

    def rows_d(e, v, j):
        def build():
            rows_at = rows_of(zat[e], 1 - y if v else y, j)
            return remote(
                rows_at, rows_at, r.nd_send.at[v], r.nd_recv.at[v, e], dev(z, x, y, 0)
            )

        return build

    def got_rows(e, v):
        view = r.normed.at[zat[e], pl.ds((1 - y if v else y) * CS, CS)]
        remote(view, view, r.nd_send.at[v], r.nd_recv.at[v, e], c_peer).wait_recv()

    go(rows_c)

    def send_down(if_outer, if_inner):
        @pl.when(outer)
        def _():
            send_weights(((2, if_outer),))

        @pl.when(jnp.logical_not(outer))
        def _():
            send_weights(((2, if_inner),))

    @pl.when(c == 1)
    def _():
        go(rows_z(0, 1))
        go(rows_y(0, 1))
        rows_c().wait_recv()
        go(rows_z(0, 0))
        for j in (1, 0):
            go(rows_z(1, j))
        go(rows_y(0, 0))

    @pl.when(c == 0)
    def _():
        rows_c().wait_recv()

    pass_if(early, ((0, 3),))
    own_copies[2].wait()
    pass_on(2, 0)
    pass_on(1, 3)

    @pl.when(c == 1)
    def _():
        for j in (1, 0):
            rows_z(1, j)().wait_recv()
            go(rows_y(1, j))
            go(rows_d(1, 0, j))
        for j in (1, 0):
            rows_y(0, j)().wait_recv()
            go(rows_d(0, 1, j))
        for j in (1, 0):
            rows_z(0, j)().wait_recv()
            go(rows_z(2, j))
            go(rows_y(2, j))
            go(rows_d(2, 0, j))

    pass_on(1, 2)
    pass_on(2, 1)

    @pl.when(c == 0)
    def _():
        got_rows(2, 0)
        send_down(2, 3)

    @pl.when(c == 1)
    def _():
        for j in (1, 0):
            rows_y(1, j)().wait_recv()
            go(rows_d(1, 1, j))
        for j in (1, 0):
            rows_z(2, j)().wait_recv()
            go(rows_y(3, j))
            go(rows_d(3, 0, j))

    @pl.when(c == 0)
    def _():
        got_rows(3, 0)
        send_down(3, 2)
        for e, v in ((1, 0), (0, 1), (1, 1)):
            got_rows(e, v)

    def project(m, half_z):
        block = r.normed[pl.ds(2 * half_z, 2)].reshape(2 * rows, r.normed.shape[3])
        total = dot_nt(block[:, :width], r.wg[m, 0])
        for s in range(1, ns):
            total += dot_nt(block[:, s * width : (s + 1) * width], r.wg[m, s])
        return total

    def gate_rows(half_z):
        gate = project(0, half_z)
        r.gated[half_z] = gate / (1.0 + jnp.exp(-gate))

    def half_at(half_z):
        return pl.ds(pl.multiple_of(half_z * 2 * rows, 2 * rows), 2 * rows)

    def hand_hidden(i):
        at = half_at(own_half if i == 0 else 1 - own_half)
        return lambda: remote(
            r.hidden.at[0, at], r.hidden.at[1, at], r.hx_send, r.hx_recv.at[i], x_peer
        )

    def up_rows(i):
        half_z = own_half if i == 0 else 1 - own_half
        r.hidden[0, half_at(half_z), :] = (r.gated[half_z] * project(1, half_z)).astype(BF16)
        go(hand_hidden(i))

    own_half = z // 2
    own_copies[0].wait()
    got_forwards(0)
    gate_rows(own_half)

    @pl.when(c == 1)
    def _():
        for e in (2, 3):
            for j in (1, 0):
                rows_y(e, j)().wait_recv()
                go(rows_d(e, 1, j))

    own_copies[1].wait()
    got_forwards(1)
    up_rows(0)

    @pl.when(c == 0)
    def _():
        for e in (2, 3):
            got_rows(e, 1)

    gate_rows(1 - own_half)
    up_rows(1)

    low = c == 0

    def t1(b, u):
        return lambda: remote(
            r.s1.at[b, u], r.r1.at[b, u], r.t1_send, r.t1_recv.at[b, u], c_peer
        )

    def t2(b, u):
        return lambda: remote(
            r.s2.at[b, u],
            r.r2.at[b, u],
            r.t2_send,
            r.t2_recv.at[b, u],
            dev(z, x, 1 - y, c),
        )

    def unit(b, u):
        return XS * b + u if b < 2 else b + 2

    def t3(b, u, e):
        if b > 1 and u:
            return lambda: remote(
                r.s3x.at[b - 2, e],
                r.r3x.at[b - 2, e],
                r.t3x_send,
                r.t3x_recv.at[b - 2],
                dev(zat[e], 1 - x, y, c),
            )
        return lambda: remote(
            r.s3.at[unit(b, u), e - 1],
            r.r3.at[unit(b, u), e - 1],
            r.t3_send,
            r.t3_recv.at[unit(b, u)],
            dev(zat[e], x, y, c),
        )

    def side(u):
        return 1 - x if u else x

    def compute(b, u):
        if b < 2:
            if u:
                forward(2, b)().wait_recv()
            part = dot_nn(r.hidden[0], r.wg[2, zat[b] * XS + side(u)])
        else:
            part = dot_nn(r.hidden[u], r.wg[2, zat[b] * XS + x])
        for zz in range(nz):
            for yy in range(nt // CS):
                at = zz * rows + yy * CS * quarter
                even = part[at : at + quarter]
                odd = part[at + quarter : at + 2 * quarter]
                r.keep[b, u, yy, zz] = jnp.where(low, even, odd)
                r.s1[b, u, yy, zz] = jnp.where(low, odd, even).astype(BF16)
        go(t1(b, u))

    def second(b, u):
        t1(b, u)().wait_recv()
        r.s2[b, u] = (r.keep[b, u, 1 - y] + r.r1[b, u, 1 - y].astype(F32)).astype(BF16)
        go(t2(b, u))
        r.keep[b, u, y] = r.keep[b, u, y] + r.r1[b, u, y].astype(F32)

    def third(b, u):
        t2(b, u)().wait_recv()
        def value(e):
            return r.keep[b, u, y, zat[e]] + r.r2[b, u, zat[e]].astype(F32)

        if b > 1 and u:
            for e in (3, 2, 1, 0):
                r.s3x[b - 2, e] = value(e).astype(BF16)
                go(t3(b, u, e))
            return
        for e in (3, 2, 1):
            r.s3[unit(b, u), e - 1] = value(e).astype(BF16)
            go(t3(b, u, e))
        r.acc[zat[b], side(u)] = r.acc[zat[b], side(u)] + value(0)

    def last(b, u):
        if b > 1 and u:
            view = r.r3x.at[b - 2]
            remote(view, view, r.t3x_send, r.t3x_recv.at[b - 2], c_peer).wait_recv()
            for e in range(nz):
                g = zat[b ^ e]
                r.acc[g, 1 - x] = r.acc[g, 1 - x] + r.r3x[b - 2, e].astype(F32)
            return
        view = r.r3.at[unit(b, u)]
        remote(view, view, r.t3_send, r.t3_recv.at[unit(b, u)], c_peer).wait_recv()
        for e in (1, 3, 2):
            g = zat[b ^ e]
            r.acc[g, side(u)] = r.acc[g, side(u)] + r.r3[unit(b, u), e - 1].astype(F32)

    def other_hidden():
        for i in range(2):
            hand_hidden(i)().wait_recv()

    for b in range(2):
        for u in range(XS):
            compute(b, u)
    for b in range(2):
        for u in range(XS):
            second(b, u)
    got_weight(2, 3)
    compute(3, 0)
    third(0, 0)
    second(3, 0)
    third(0, 1)
    got_weight(2, 2)
    compute(2, 0)
    other_hidden()
    compute(3, 1)
    compute(2, 1)
    third(1, 0)
    second(2, 0)
    second(3, 1)
    second(2, 1)
    third(1, 1)
    third(3, 0)
    third(2, 0)
    third(3, 1)
    third(2, 1)
    for b in (0, 1):
        for u in range(XS):
            last(b, u)
    for b, u in ((3, 0), (2, 0), (3, 1), (2, 1)):
        last(b, u)
    for g in range(nz):
        for u in range(XS):
            at = g * group + u * width
            r.out[:, at : at + width] = r.acc[g, u].astype(BF16)

    sent(r.wg.at[:2, : nz + 1], r.f_send)
    sent(r.hidden.at[0], r.hx_send)
    sent(r.s1, r.t1_send)
    sent(r.s2, r.t2_send)
    sent(r.s3, r.t3_send)
    sent(r.s3x, r.t3x_send)
    for build in (cross_c(c), cross_t(c), rows_c, mix_c, mix_y):
        build().wait_send()

    @pl.when(c == 0)
    def _():
        sent(r.wg.at[:, : CS * (nz - 1)], r.w_send)
        near_c().wait_send()
        near_t().wait_send()

    @pl.when(c == 1)
    def _():
        sent(r.slab, r.h_send)
        sent(r.normed.at[:3, :CS], r.nz_send)
        sent(r.normed.at[:CS], r.ny_send)
        sent(r.normed.at[: nz - 1, :CS], r.nd_send.at[0])
        sent(r.normed.at[:CS], r.nd_send.at[1])
        for build in (state_x(0), state_x(1), state_c):
            build().wait_send()

    @pl.when(jnp.logical_and(c == 1, z < nz - 1))
    def _():
        chain().wait_send()


def fast_body(
    queries,
    key_rows,
    value_rows,
    gate_input,
    log_decay,
    head_gain,
    out_weight,
    residual,
    mlp_gain,
    gate_weight,
    up_weight,
    down_weight,
):
    rows, wide = queries.shape
    heads = log_decay.shape[1]
    hd = wide // heads
    model = residual.shape[1]
    ns, nt = lax.axis_size("sp"), lax.axis_size("tp")
    nz = ns // XS
    quarter = rows // nt
    width, units = gate_weight.shape
    share = units // nz
    hh = heads // XS
    vmem = pltpu.VMEM
    dma = pltpu.SemaphoreType.DMA
    operands = {
        "q_hbm": queries,
        "k_hbm": key_rows,
        "v_hbm": value_rows,
        "g_hbm": gate_input,
        "ld_hbm": log_decay.T,
        "hg_hbm": head_gain.reshape(1, wide),
        "res_hbm": residual,
        "mg_hbm": mlp_gain.reshape(1, model),
        "ow_hbm": out_weight,
        "gw_hbm": gate_weight,
        "uw_hbm": up_weight,
        "dw_hbm": down_weight,
    }
    scratch = {
        "q": vmem((rows, wide), BF16),
        "k": vmem((rows, wide), BF16),
        "v": vmem((rows, wide), BF16),
        "g": vmem((rows, wide), BF16),
        "ld": vmem((heads, rows), F32),
        "hg": vmem((1, wide), F32),
        "res": vmem((quarter, model), BF16),
        "mg": vmem((1, model), F32),
        "ow": vmem(out_weight.shape, BF16),
        "raw": vmem((2, width, units), BF16),
        "slab": vmem((3, units, width), BF16),
        "partner": vmem((3, units, width), BF16),
        "wg": vmem((3, ns, share, width), BF16),
        "qrot": vmem((rows, wide), BF16),
        "inner": vmem((rows, wide), F32),
        "cumx": vmem((rows, wide), F32),
        "c_out": vmem((heads, hd, hd), BF16),
        "t_out": vmem((heads, 8, hd), F32),
        "ci": vmem((XS, CS, hh, hd, hd), BF16),
        "ti": vmem((XS, CS, hh, 8, hd), F32),
        "plane": vmem((CS, hh, hd, hd), F32),
        "ch_in": vmem((CS, hh, hd, hd), BF16),
        "ch_out": vmem((CS, hh, hd, hd), BF16),
        "so": vmem((XS, CS, hh, hd, hd), BF16),
        "s_in": vmem((XS, hh, hd, hd), BF16),
        "retained": vmem((rows, wide), BF16),
        "mc_out": vmem((nt // CS, quarter, model), BF16),
        "mc_in": vmem((nt // CS, quarter, model), BF16),
        "mix_own": vmem((nt // CS, quarter, model), F32),
        "my_out": vmem((quarter, model), BF16),
        "my_in": vmem((quarter, model), BF16),
        "acc": vmem((nz, XS, quarter, width), F32),
        "normed": vmem((nz, nt, quarter, model), BF16),
        "gated": vmem((nz // 2, 2 * rows, share), F32),
        "hidden": vmem((XS, nz * rows, share), BF16),
        "keep": vmem((nz, XS, nt // CS, nz, quarter, width), F32),
        "s1": vmem((nz, XS, nt // CS, nz, quarter, width), BF16),
        "r1": vmem((nz, XS, nt // CS, nz, quarter, width), BF16),
        "s2": vmem((nz, XS, nz, quarter, width), BF16),
        "r2": vmem((nz, XS, nz, quarter, width), BF16),
        "s3": vmem((nz + 2, nz - 1, quarter, width), BF16),
        "r3": vmem((nz + 2, nz - 1, quarter, width), BF16),
        "s3x": vmem((2, nz, quarter, width), BF16),
        "r3x": vmem((2, nz, quarter, width), BF16),
        "in_sem": dma((len(operands),)),
        "own_sem": dma((3,)),
        "h_send": dma,
        "h_recv": dma((3,)),
        "w_send": dma,
        "w_recv": dma((3, nz - 1)),
        "f_send": dma,
        "f_recv": dma((4,)),
        "cx_send": dma((2,)),
        "cx_recv": dma((2, CS)),
        "cc_send": dma((2,)),
        "cc_recv": dma((2,)),
        "ch_send": dma,
        "ch_recv": dma,
        "so_send": dma((3,)),
        "s_recv": dma((XS,)),
        "mix_send": dma((2,)),
        "mix_recv": dma((2,)),
        "nc_send": dma,
        "nc_recv": dma,
        "nz_send": dma,
        "nz_recv": dma((3, CS)),
        "ny_send": dma,
        "ny_recv": dma((nz, CS)),
        "nd_send": dma((2,)),
        "nd_recv": dma((2, nz)),
        "t1_send": dma,
        "t1_recv": dma((nz, XS)),
        "t2_send": dma,
        "t2_recv": dma((nz, XS)),
        "t3_send": dma,
        "t3_recv": dma((nz + 2,)),
        "t3x_send": dma,
        "t3x_recv": dma((2,)),
        "hx_send": dma,
        "hx_recv": dma((2,)),
    }
    names = list(operands) + ["out"] + list(scratch)
    return pl.pallas_call(
        functools.partial(kernel, names, nz, nt),
        out_shape=pltpu.VMEM((quarter, model), BF16),
        in_specs=[pl.BlockSpec(memory_space=pl.ANY)] * len(operands),
        out_specs=pl.BlockSpec(memory_space=pltpu.VMEM),
        scratch_shapes=list(scratch.values()),
        compiler_params=pltpu.CompilerParams(
            collective_id=0, has_side_effects=True, vmem_limit_bytes=60 * 1024 * 1024
        ),
    )(*operands.values())


def fits(mesh, queries, log_decay, gate_weight):
    ns, nt = mesh.shape["sp"], mesh.shape["tp"]
    tokens, wide = queries.shape
    if ns % XS or ns // XS != 4 or nt != 2 * CS or tokens // ns != BLOCK:
        return False
    nz = ns // XS
    hidden = gate_weight.shape[1] // nt
    return (
        gate_weight.shape[0] // ns % 128 == 0
        and hidden % (16 * nz) == 0
        and wide // log_decay.shape[1] == 128
        and BLOCK % (16 * nt) == 0
        and hidden % 128 == 0
        and log_decay.shape[1] // nt % XS == 0
    )


def solution(mesh):
    def run(*args):
        good = fits(mesh, args[0], args[4], args[9])
        return jax.shard_map(
            fast_body if good else body,
            mesh=mesh,
            in_specs=(
                P("sp", "tp"),
                P("sp", "tp"),
                P("sp", "tp"),
                P("sp", "tp"),
                P("sp", "tp"),
                P("tp"),
                P("tp", None),
                P("sp", None),
                P(),
                P("sp", "tp"),
                P("sp", "tp"),
                P("tp", "sp"),
            ),
            out_specs=P(("sp", "tp"), None),
            check_vma=False,
        )(*args)

    return run
```
